1024 devices in a mesh: ep: 64 (over z, y), tp: 16 (over x, core).
Axes of the slice: x: 8, y: 8, z: 8, core: 2. Of those that a mesh axis runs over, the one named last changes fastest.
Arguments:
- tokens: bfloat16 [2048, 4096], P('ep', 'tp')
- norm_gain: float32 [4096], P('tp'), may hold values from 0.1 to 1.9
- routes: int32 [2048, 8], P('ep'), may hold values from 0 to 63, all different within a row; in each aligned block of 32 rows (0 to 31, 32 to 63, ...) at most 6 rows name the same one
- route_weights: float32 [2048, 8], P('ep'), may hold values from 0.1 to 1
- gate_proj: bfloat16 [64, 4096, 1024], P('ep', 'tp'), may hold values from -0.09375 to 0.09375
- up_proj: bfloat16 [64, 4096, 1024], P('ep', 'tp'), may hold values from -0.09375 to 0.09375
- down_proj: bfloat16 [64, 1024, 4096], P('ep', None, 'tp')
- shared_gate: bfloat16 [4096, 1024], P('tp'), may hold values from -0.09375 to 0.09375
- shared_up: bfloat16 [4096, 1024], P('tp'), may hold values from -0.09375 to 0.09375
- shared_down: bfloat16 [1024, 4096], P(None, 'tp')
- out_gain: float32 [4096], P('tp'), may hold values from 0.1 to 1.9
Outputs:
- mixed_out: bfloat16 [2048, 4096], P('ep', 'tp')
The draws below stay inside these ranges and needn't reach their ends.
Inputs may be any that keep to these rules, and one draw needn't show every extreme that they name: `routes`: among the 32 rows of one device no expert is named more than 6 times, and in every draw some expert is named exactly 6 times by the rows of some device.
All inputs are finite; a program needn't handle non-finite values.
Results may differ from the reference program's by a relative error of at most 0.028.
Values may be sent and summed in bfloat16 or wider, within the bound.
No kernel may reach another device: no remote copies, remote signals or barrier semaphores. Data moves between devices by JAX's collectives and lax.ppermute only.
A program may use at most 32 MiB of HBM per device.

```python
import math
import jax
import jax.numpy as jnp
import numpy as np
from jax import lax

D = 4096
F = 1024
FS = 1024
TOP_K = 8
TOK_DEV = 32
EXPERTS = 64
CAP = 6
TOKENS = 2048
N_EP = 64
N_TP = 16


def column_scales(key, length):
    rising = jnp.exp(jnp.linspace(0.0, math.log(6.0), length))
    return rising * jax.random.uniform(key, (length,), jnp.float32, 0.5, 1.5)


def draw_tokens(key, part):
    key_base = jax.random.fold_in(key, 11)
    key_rows = jax.random.fold_in(key, 12)
    key_cols = jax.random.fold_in(key, 13)
    values = jax.random.normal(key_base, (TOKENS, D), jnp.float32)
    row_scale = jnp.exp(jax.random.uniform(key_rows, (TOKENS, 1), jnp.float32, 0.0, math.log(10.0)))
    return (values * row_scale * column_scales(key_cols, D)[None, :]).astype(jnp.bfloat16)


def down_values(key, shape):
    key_base = jax.random.fold_in(key, 21)
    key_cols = jax.random.fold_in(key, 22)
    values = jax.random.normal(key_base, shape, jnp.float32)
    return values * shape[-2] ** (-0.5) * column_scales(key_cols, D)


def draw_down_proj(key, part):
    return down_values(key, (EXPERTS, F, D)).astype(jnp.bfloat16)


def draw_shared_down(key, part):
    return down_values(key, (FS, D)).astype(jnp.bfloat16)


def block_scale(own_key, shape, cuts, least, largest):
    level, own = 1.0, jax.random.fold_in(own_key, 6)
    for dim, blocks in cuts:
        heights = jnp.exp(jax.random.uniform(jax.random.fold_in(own, dim), (blocks,), jnp.float32, least / len(cuts), largest / len(cuts)))
        level = level * jnp.repeat(heights, shape[dim] // blocks).reshape([-1 if axis == dim else 1 for axis in range(len(shape))])
    return level


def shared_out(own_key, own, number, rows, count, top, most, lean):
    order = jax.random.permutation(own_key, count)
    packed, usual = load_shares(count, rows * top, most, lean, True), load_shares(count, rows * top, most, lean, False)
    places = jnp.arange(count)

    def named(sizes, rotation):
        used = int((sizes > 0).sum())
        fixed = max(1, used // 4)
        moved = fixed + (places - fixed + rotation * (used - fixed)) % max(1, count - fixed)
        return jnp.zeros((count,), jnp.int32).at[order[jnp.where(places < fixed, places, moved)]].set(jnp.asarray(sizes, jnp.int32))

    sizes = jnp.where(number % 4 == 0, named(packed, number // 4), named(usual, number - number // 4 - 1))
    mixed = jax.random.permutation(jax.random.fold_in(own, 3), count)
    giver, receiver = mixed[0:count // 2 * 2:2], mixed[1:count // 2 * 2:2]
    margin = jnp.minimum(sizes[giver] - 1, most - sizes[receiver]) // 2
    margin = jnp.where((giver == order[0]) | (receiver == order[0]) | (sizes[receiver] == 0), 0, jnp.maximum(margin, 0))
    moved = jax.random.randint(jax.random.fold_in(own, 4), (count // 2,), 0, 1 << 20) % (margin + 1)
    sizes = sizes.at[giver].add(-moved).at[receiver].add(moved)
    items = jnp.searchsorted(jnp.cumsum(sizes), jnp.arange(rows * top), side="right").astype(jnp.int32)
    table = items.reshape(top, rows).T
    table = table[jax.random.permutation(jax.random.fold_in(own, 1), rows)]
    rotation = jax.random.randint(jax.random.fold_in(own, 2), (rows, 1), 0, top)
    return jnp.take_along_axis(table, (jnp.arange(top)[None, :] + rotation) % top, axis=1)


def load_shares(number_of, total, bound, lean, full):
    weights = [(1 << 20) // math.isqrt(grade ** lean) + 1 for grade in range(1, number_of + 1)]
    largest = bound if full else min(bound, max(-(-total // number_of), total * weights[0] // sum(weights)))
    least = 1 if total - largest >= number_of - 1 else 0
    counts, surplus = [largest] + [least] * (number_of - 1), total - largest - least * (number_of - 1)
    while surplus > 0:
        free = [i for i in range(1, number_of) if counts[i] < largest] or [i for i in range(1, number_of) if counts[i] < bound]
        whole, budget = sum([weights[i] for i in free]), surplus
        for i in free:
            addition = min(bound - counts[i], max(1, budget * weights[i] // whole), surplus)
            counts[i] = counts[i] + addition
            surplus = surplus - addition
    return np.array(counts)


def bell_draw(key, shape, width, most, shards=(), kind=jnp.bfloat16):
    array = jax.random.normal(key, shape, jnp.float32) * width
    if len(shards) > 0:
        array = block_scale(key, shape, shards, -0.22, 0.18) * array
    return jnp.clip(array, min=-most, max=most).astype(kind)


def setup_inputs(seed: int = 0) -> dict:
    streams_of = jax.random.split(jax.random.key(seed), 12)
    tokens = draw_tokens(jax.random.fold_in(streams_of[11], 71), 0)
    norm_gain = jnp.clip(1.0 + 0.18 * jax.random.normal(streams_of[1], (D,), jnp.float32), 0.1, 1.9)
    routes_keys = jax.random.split(jax.random.fold_in(streams_of[2], 1), TOKENS // TOK_DEV)
    routes_turns = jax.random.permutation(jax.random.fold_in(streams_of[2], 3), TOKENS // TOK_DEV)
    routes = jax.vmap(lambda own, number: shared_out(jax.random.fold_in(streams_of[2], 2), own, number, TOK_DEV, EXPERTS, TOP_K, CAP, 2))(routes_keys, routes_turns).reshape((TOKENS, TOP_K))
    route_weights = jnp.clip(jnp.exp(math.log(1.0) - 2.3025851 * jax.random.uniform(streams_of[3], (TOKENS, TOP_K), jnp.float32) ** block_scale(streams_of[3], (TOKENS, TOP_K), ((0, 64),), -0.2, 0.2)), 0.1, 1.0)
    gate_proj = bell_draw(streams_of[4], (EXPERTS, D, F), D ** -0.5, 0.09375, ((0, 64), (1, 16)))
    up_proj = bell_draw(streams_of[5], (EXPERTS, D, F), D ** -0.5, 0.09375, ((0, 64), (1, 16)))
    down_proj = draw_down_proj(jax.random.fold_in(streams_of[11], 71), 0)
    shared_gate = bell_draw(streams_of[7], (D, FS), D ** -0.5, 0.09375, ((0, 16),))
    shared_up = bell_draw(streams_of[8], (D, FS), D ** -0.5, 0.09375, ((0, 16),))
    shared_down = draw_shared_down(jax.random.fold_in(streams_of[11], 71), 0)
    out_gain = jnp.clip(1.0 + 0.18 * jax.random.normal(streams_of[10], (D,), jnp.float32), 0.1, 1.9)
    return {"tokens": tokens, "norm_gain": norm_gain, "routes": routes, "route_weights": route_weights, "gate_proj": gate_proj, "up_proj": up_proj, "down_proj": down_proj, "shared_gate": shared_gate, "shared_up": shared_up, "shared_down": shared_down, "out_gain": out_gain}


def split_product(left_rows, weight):
    row_count = left_rows.shape[0]
    out_width = weight.shape[1]
    left_side = left_rows.astype(jnp.float32).reshape(row_count, N_TP, D // N_TP)
    right_side = weight.astype(jnp.float32).reshape(N_TP, D // N_TP, out_width)
    partial_value = jnp.einsum('rtd,tdf->rtf', left_side, right_side).astype(jnp.bfloat16)
    partial_value = lax.optimization_barrier(partial_value).astype(jnp.float32)
    return lax.optimization_barrier(jnp.sum(partial_value, axis=1))

def swiglu(gate_pre, up_pre):
    return (jax.nn.silu(gate_pre) * up_pre).astype(jnp.bfloat16)

def reference(tokens, norm_gain, routes, route_weights, gate_proj, up_proj, down_proj, shared_gate, shared_up, shared_down, out_gain):
    tokens_f = tokens.astype(jnp.float32)
    scale = lax.rsqrt(lax.optimization_barrier(jnp.mean(tokens_f * tokens_f, axis=1, keepdims=True)) + 1e-06)
    normed = (tokens_f * scale * norm_gain[None, :]).astype(jnp.bfloat16)
    shared_hidden = swiglu(split_product(normed, shared_gate), split_product(normed, shared_up))
    shared_part = jnp.dot(shared_hidden, shared_down, preferred_element_type=jnp.float32)
    chosen = jnp.concatenate([routes.reshape(-1), jnp.full((1,), -1, jnp.int32)])
    weight_list = jnp.concatenate([route_weights.reshape(-1), jnp.zeros((1,), jnp.float32)])
    token_list = jnp.concatenate([jnp.arange(TOKENS * TOP_K, dtype=jnp.int32) // TOP_K, jnp.zeros((1,), jnp.int32)])
    row_limit = N_EP * CAP
    sentinel = TOKENS * TOP_K

    def add_expert(totals, expert):
        picked = jnp.nonzero(chosen == expert, size=row_limit, fill_value=sentinel)[0].astype(jnp.int32)
        rows_of = token_list[picked]
        chosen_rows = normed[rows_of]
        hidden = swiglu(split_product(chosen_rows, gate_proj[expert]), split_product(chosen_rows, up_proj[expert]))
        result = jnp.dot(hidden, down_proj[expert], preferred_element_type=jnp.float32).astype(jnp.bfloat16)
        result = lax.optimization_barrier(result).astype(jnp.float32)
        totals = totals.at[rows_of].add(result * weight_list[picked][:, None])
        return (totals, None)
    routed, _ = lax.scan(add_expert, jnp.zeros((TOKENS, D), jnp.float32), jnp.arange(EXPERTS, dtype=jnp.int32))
    mixed = shared_part + routed
    final_scale = lax.rsqrt(lax.optimization_barrier(jnp.mean(mixed * mixed, axis=1, keepdims=True)) + 1e-06)
    return (mixed * final_scale * out_gain[None, :]).astype(jnp.bfloat16)
```

```python
import jax
import jax.numpy as jnp
from jax import lax
from jax.experimental import pallas as pl
from jax.experimental.pallas import tpu as pltpu
from jax.sharding import Mesh, PartitionSpec as P

D = 4096
EPS = 1e-06
bf16, f32, i32 = jnp.bfloat16, jnp.float32, jnp.int32
MIB = 1024 * 1024


def iota(shape, dim):
    return lax.broadcasted_iota(i32, shape, dim)


def dot(a, b):
    return jnp.dot(a, b, preferred_element_type=f32)


def to_row(column, lanes):
    rows = column.shape[0]
    own = iota((rows, lanes), 0) == iota((rows, lanes), 1)
    return jnp.sum(jnp.where(own, column, 0.0), axis=0, keepdims=True)


def to_column(row, rows):
    lanes = row.shape[1]
    own = iota((rows, lanes), 0) == iota((rows, lanes), 1)
    return jnp.sum(jnp.where(own, row, 0.0), axis=1, keepdims=True)


def three_parts(value):
    high = value.astype(bf16).astype(f32)
    rest = jnp.where(high < jnp.inf, value - high, 0.0)
    middle = rest.astype(bf16).astype(f32)
    return high, middle, rest - middle


def named_slots(routes, lanes):
    rows, picks = routes.shape
    expert = iota((rows, lanes), 1) >> 3
    named = routes[:, 0:1] == expert
    for k in range(1, picks):
        named = named | (routes[:, k : k + 1] == expert)
    earlier = (iota((rows, rows), 1) < iota((rows, rows), 0)).astype(f32).astype(bf16)
    rank = dot(earlier, jnp.where(named, 1.0, 0.0).astype(bf16))
    return named, rank.astype(i32)


def pack_kernel(core_ref, routes_ref, own_ref, both_ref, out_ref):
    core = core_ref[0]
    lanes = out_ref.shape[0]
    named, rank = named_slots(routes_ref[...], lanes)
    lane = iota(named.shape, 1)
    slot = lane & 3
    chosen = named & (rank == 3 * core + slot) & (slot < 3)
    other = (lane & 4) > 0
    picks = jnp.concatenate(
        [
            jnp.where(chosen & ~other, 1.0, 0.0).astype(bf16),
            jnp.where(chosen & other, 1.0, 0.0).astype(bf16),
        ],
        axis=0,
    )
    rows = jnp.concatenate([own_ref[...], both_ref[1 - core]], axis=0)
    out_ref[...] = lax.dot_general(
        picks, rows, (((0,), (0,)), ((), ())), preferred_element_type=f32
    ).astype(bf16)


def weights_kernel(routes_ref, weights_ref, out_ref):
    routes = routes_ref[...]
    lanes = out_ref.shape[2]
    named, rank = named_slots(routes, lanes)
    lane = iota(named.shape, 1)
    weight = jnp.zeros(named.shape, f32)
    for k in range(routes.shape[1]):
        weight = jnp.where(routes[:, k : k + 1] == lane >> 3, weights_ref[:, k : k + 1], weight)
    weight = jnp.where(named & (rank == (lane & 7)), weight, 0.0)
    for n, part in enumerate(three_parts(weight)):
        out_ref[n] = part.astype(bf16)


def shared_up_kernel(core_ref, own_ref, gain_ref, gate_ref, up_ref, keep_ref, send_ref):
    first = core_ref[0] == 0
    rows = (own_ref[...].astype(f32) * gain_ref[...]).astype(bf16)
    half = rows.shape[0] // 2
    for n in range(keep_ref.shape[0]):
        cut = slice(n * 128, (n + 1) * 128)
        part = dot(rows, jnp.concatenate([gate_ref[:, cut], up_ref[:, cut]], axis=1))
        keep_ref[n] = jnp.where(first, part[:half], part[half:])
        send_ref[n] = jnp.where(first, part[half:], part[:half]).astype(bf16)


def hidden_parts_kernel(
    core_ref,
    rows_ref,
    both_ref,
    gain_ref,
    gain_other_ref,
    gate_ref,
    up_ref,
    gate_other_ref,
    up_other_ref,
    kept_ref,
    sent_ref,
    out_ref,
):
    first = core_ref[0] == 0
    arrived = rows_ref[...]
    slots = 3 * arrived.shape[0] // 8
    sources = arrived.shape[0] // 8
    to, at = iota((slots, arrived.shape[0]), 0), iota((slots, arrived.shape[0]), 1)
    place = (to % sources) * 8 + to // sources
    own = dot(jnp.where(at == place, 1.0, 0.0).astype(bf16), arrived)
    other = dot(jnp.where(at == place + 4, 1.0, 0.0).astype(bf16), arrived)
    squares = jnp.sum(own * own + other * other, axis=1, keepdims=True)
    near, far = both_ref[0].astype(f32), both_ref[1].astype(f32)
    token_squares = jnp.sum(near * near + far * far, axis=1, keepdims=True)
    half = token_squares.shape[0] // 2
    token_squares = jnp.where(first, token_squares[:half], token_squares[half:])
    squares = jnp.concatenate([squares, token_squares], axis=0) * (1.0 / D)
    parts = three_parts(to_row(squares, 256))
    line = iota((8, 256), 0)
    extra = jnp.where(line == 0, parts[0], jnp.where(line == 1, parts[1], parts[2]))
    extra = jnp.where(line < 3, extra, 0.0).astype(bf16)
    own = (own * gain_ref[...]).astype(bf16)
    other = (other * gain_other_ref[...]).astype(bf16)
    for n in range(out_ref.shape[0]):
        cut = slice(n * 128, (n + 1) * 128)
        part = dot(own, jnp.concatenate([gate_ref[:, cut], up_ref[:, cut]], axis=1)) + dot(
            other, jnp.concatenate([gate_other_ref[:, cut], up_other_ref[:, cut]], axis=1)
        )
        out_ref[n, :slots] = part.astype(bf16)
        out_ref[n, slots : slots + half] = (kept_ref[n] + sent_ref[n].astype(f32)).astype(bf16)
        out_ref[n, slots + half :] = extra


def hidden_kernel(parts_ref, out_ref):
    rows = out_ref.shape[0]
    total = parts_ref[0].astype(f32)
    for n in range(1, parts_ref.shape[0]):
        total = total + parts_ref[n].astype(f32)
    mean = total[rows : rows + 1] + total[rows + 1 : rows + 2] + total[rows + 2 : rows + 3]
    scale = to_column(lax.rsqrt(mean + EPS), rows)
    gate = jnp.where(scale > 0.0, total[:rows, :128] * scale, 0.0)
    up = jnp.where(scale > 0.0, total[:rows, 128:] * scale, 0.0)
    out_ref[...] = (gate / (1.0 + jnp.exp(-gate)) * up).astype(bf16)


def lanes_of(ref, core, lo, hi):
    return jnp.concatenate([ref[n, lo:hi] for n in range(core, ref.shape[0], 2)], axis=1)


def down_kernel(hidden_ref, down_ref, out_ref):
    sent = out_ref.shape[0]
    slots = 3 * sent // 8
    down = down_ref[...]
    rows = jnp.concatenate(
        [dot(lanes_of(hidden_ref, core, 0, slots), down).astype(bf16) for core in range(2)], axis=0
    )
    to, at = iota((sent, 2 * slots), 0), iota((sent, 2 * slots), 1)
    place = (to & 7) * (sent // 8) + (to >> 3)
    out_ref[...] = dot(jnp.where(at == place, 1.0, 0.0).astype(bf16), rows).astype(bf16)


def shared_down_kernel(hidden_ref, down_ref, out_ref):
    rows = hidden_ref.shape[1]
    half = out_ref.shape[0] // 2
    hidden = jnp.concatenate(
        [lanes_of(hidden_ref, core, rows - half, rows) for core in range(2)], axis=0
    )
    out_ref[...] = dot(hidden, down_ref[...])


def combine_kernel(rows_ref, weights_ref, shared_ref, mixed_ref, squares_ref):
    rows = rows_ref[...]
    mixed = shared_ref[...]
    for n in range(3):
        mixed = mixed + dot(weights_ref[n], rows)
    mixed_ref[...] = mixed
    squares = to_row(jnp.sum(mixed * mixed, axis=1, keepdims=True), 128)
    squares_ref[...] = jnp.broadcast_to(squares[None], squares_ref.shape)


def norm_kernel(squares_ref, mixed_ref, gain_ref, out_ref):
    total = jnp.sum(squares_ref[...], axis=0)
    scale = to_column(lax.rsqrt(total / D + EPS), out_ref.shape[0])
    out_ref[...] = (mixed_ref[...] * scale * gain_ref[...]).astype(bf16)


def call(body, out, *operands, flops=0):
    def spec(array):
        return pl.BlockSpec(memory_space=pltpu.SMEM if array.shape == (1,) else pltpu.VMEM)

    outs = out if isinstance(out, tuple) else (out,)
    specs = tuple(pl.BlockSpec(memory_space=pltpu.VMEM) for _ in outs)
    moved = sum(a.size * a.dtype.itemsize for a in (*operands, *outs))
    return pl.pallas_call(
        body,
        out_shape=out,
        in_specs=[spec(a) for a in operands],
        out_specs=specs if isinstance(out, tuple) else specs[0],
        compiler_params=pltpu.CompilerParams(vmem_limit_bytes=24 * MIB),
        cost_estimate=pl.CostEstimate(flops=flops, bytes_accessed=moved, transcendentals=0),
        name=body.__name__,
    )(*operands)


def shape(dims, dtype):
    return jax.ShapeDtypeStruct(dims, dtype)


def per_device(
    tokens,
    norm_gain,
    routes,
    route_weights,
    gate_proj,
    up_proj,
    down_proj,
    shared_gate,
    shared_up,
    shared_down,
    out_gain,
):
    rows, features = tokens.shape
    sources, lines, cores = (lax.axis_size(a) for a in ("ep", "x", "core"))
    sent = sources * 8
    slots = sources * 3
    half = rows // 2
    core = lax.axis_index("core").astype(i32).reshape(1)
    swap = [(0, 1), (1, 0)]
    gain = norm_gain.reshape(1, features)
    gate, up, down = gate_proj[0], up_proj[0], down_proj[0]

    both = lax.all_gather(tokens, "core", axis=0)
    outgoing = call(pack_kernel, shape((sent, features), bf16), core, routes, tokens, both)
    arrived = lax.all_to_all(outgoing.reshape(sources, 8, features), "ep", 0, 0, tiled=True)

    gate_other, up_other = lax.ppermute(gate, "core", swap), lax.ppermute(up, "core", swap)
    gain_other = lax.ppermute(gain, "core", swap)
    kept, given = call(
        shared_up_kernel,
        (shape((lines, half, 256), f32), shape((lines, half, 256), bf16)),
        core,
        tokens,
        gain,
        shared_gate,
        shared_up,
        flops=2 * rows * features * 2048,
    )
    taken = lax.ppermute(given, "core", swap)

    parts = call(
        hidden_parts_kernel,
        shape((lines, slots + half + 8, 256), bf16),
        core,
        arrived.reshape(sent, features),
        both,
        gain,
        gain_other,
        gate,
        up,
        gate_other,
        up_other,
        kept,
        taken,
        flops=4 * slots * features * 2048,
    )
    parts = lax.all_to_all(parts, "x", 0, 0, tiled=True)
    hidden = call(hidden_kernel, shape((slots + half, 128), bf16), parts)
    hidden = lax.all_gather(hidden, ("x", "core"), axis=0)
    leaving = call(
        down_kernel, shape((sent, features), bf16), hidden, down, flops=4 * slots * 1024 * features
    )
    returned = lax.all_to_all(leaving.reshape(sources, 8, features), "ep", 0, 0, tiled=True)
    shared = call(
        shared_down_kernel,
        shape((rows, features), f32),
        hidden,
        shared_down,
        flops=2 * rows * 1024 * features,
    )
    weights = call(weights_kernel, shape((3, rows, sent), bf16), routes, route_weights)
    mixed, squares = call(
        combine_kernel,
        (shape((rows, features), f32), shape((lines * cores, 1, 128), f32)),
        returned.reshape(sent, features),
        weights,
        shared,
    )
    squares = lax.all_to_all(squares, ("x", "core"), 0, 0, tiled=True)
    return call(
        norm_kernel,
        shape((rows, features), bf16),
        squares,
        mixed,
        out_gain.reshape(1, features),
    )


def solution(mesh):
    sources, members = mesh.devices.shape
    inner = Mesh(mesh.devices.reshape(sources, members // 2, 2), ("ep", "x", "core"))
    tp = ("x", "core")
    return jax.shard_map(
        per_device,
        mesh=inner,
        in_specs=(
            P("ep", tp),
            P(tp),
            P("ep", None),
            P("ep", None),
            P("ep", tp, None),
            P("ep", tp, None),
            P("ep", None, tp),
            P(tp, None),
            P(tp, None),
            P(None, tp),
            P(tp),
        ),
        out_specs=P("ep", tp),
        check_vma=False,
    )
```

```python
import jax
import jax.numpy as jnp
from jax import lax
from jax.experimental import pallas as pl
from jax.experimental.pallas import tpu as pltpu
from jax.sharding import Mesh, PartitionSpec as P


D = 4096
EPS = 1e-06
bf16, f32, i32 = jnp.bfloat16, jnp.float32, jnp.int32
MIB = 1024 * 1024


def iota(shape, dim):
    return lax.broadcasted_iota(i32, shape, dim)


def dot(a, b):
    return jnp.dot(a, b, preferred_element_type=f32)


def to_row(column, lanes):
    rows = column.shape[0]
    own = iota((rows, lanes), 0) == iota((rows, lanes), 1)
    return jnp.sum(jnp.where(own, column, 0.0), axis=0, keepdims=True)


def to_column(row, rows):
    lanes = row.shape[1]
    own = iota((rows, lanes), 0) == iota((rows, lanes), 1)
    return jnp.sum(jnp.where(own, row, 0.0), axis=1, keepdims=True)


def three_parts(value):
    high = value.astype(bf16).astype(f32)
    rest = jnp.where(high < jnp.inf, value - high, 0.0)
    middle = rest.astype(bf16).astype(f32)
    return high, middle, rest - middle


def named_slots(routes, lanes):
    rows, picks = routes.shape
    expert = iota((rows, lanes), 1) >> 3
    named = routes[:, 0:1] == expert
    for k in range(1, picks):
        named = named | (routes[:, k : k + 1] == expert)
    earlier = (iota((rows, rows), 1) < iota((rows, rows), 0)).astype(f32).astype(bf16)
    rank = dot(earlier, jnp.where(named, 1.0, 0.0).astype(bf16))
    return named, rank.astype(i32)


def pack_kernel(core_ref, routes_ref, both_ref, out_ref):
    core = core_ref[0]
    lanes = out_ref.shape[0]
    named, rank = named_slots(routes_ref[...].T, lanes)
    lane = iota(named.shape, 1)
    slot = lane & 3
    chosen = named & (rank == 3 * core + slot) & (slot < 3)
    other = (lane & 4) > 0
    picks = jnp.concatenate(
        [
            jnp.where(chosen & ~other, 1.0, 0.0).astype(bf16),
            jnp.where(chosen & other, 1.0, 0.0).astype(bf16),
        ],
        axis=0,
    )
    rows = jnp.concatenate([both_ref[core], both_ref[1 - core]], axis=0)
    out_ref[...] = lax.dot_general(
        picks, rows, (((0,), (0,)), ((), ())), preferred_element_type=f32
    ).astype(bf16)


def combine_weights(routes_ref, weights_ref, out_ref):
    routes, given = routes_ref[...].T, weights_ref[...].T
    lanes = out_ref.shape[2]
    named, rank = named_slots(routes, lanes)
    lane = iota(named.shape, 1)
    weight = jnp.zeros(named.shape, f32)
    for k in range(routes.shape[1]):
        weight = jnp.where(routes[:, k : k + 1] == lane >> 3, given[:, k : k + 1], weight)
    weight = jnp.where(named & (rank == (lane & 7)), weight, 0.0)
    for n, part in enumerate(three_parts(weight)):
        out_ref[n] = part.astype(bf16)


def shared_up_kernel(
    core_ref,
    both_ref,
    gain_ref,
    gate_ref,
    up_ref,
    routes_ref,
    weights_ref,
    out_gain_ref,
    keep_ref,
    send_ref,
    combine_ref,
    later_gain_ref,
):
    later_gain_ref[...] = out_gain_ref[...]
    combine_weights(routes_ref, weights_ref, combine_ref)
    first = core_ref[0] == 0
    rows = (both_ref[core_ref[0]].astype(f32) * gain_ref[...]).astype(bf16)
    half = rows.shape[0] // 2
    for n in range(keep_ref.shape[0]):
        cut = slice(n * 128, (n + 1) * 128)
        part = dot(rows, jnp.concatenate([gate_ref[:, cut], up_ref[:, cut]], axis=1))
        keep_ref[n] = jnp.where(first, part[:half], part[half:])
        send_ref[n] = jnp.where(first, part[half:], part[:half]).astype(bf16)
    parts = three_parts(gain_ref[...])
    line = iota(send_ref.shape[1:], 0)
    gain = jnp.where(line == 0, parts[0], jnp.where(line == 1, parts[1], parts[2]))
    send_ref[keep_ref.shape[0]] = jnp.where(line < 3, gain, 0.0).astype(bf16)


def hidden_parts_kernel(
    core_ref,
    rows_ref,
    both_ref,
    gain_ref,
    gate_ref,
    up_ref,
    gate_other_ref,
    up_other_ref,
    kept_ref,
    sent_ref,
    out_ref,
):
    first = core_ref[0] == 0
    arrived = rows_ref[...]
    slots = 3 * arrived.shape[0] // 8
    sources = arrived.shape[0] // 8
    to, at = iota((slots, arrived.shape[0]), 0), iota((slots, arrived.shape[0]), 1)
    place = (to % sources) * 8 + to // sources
    own = dot(jnp.where(at == place, 1.0, 0.0).astype(bf16), arrived)
    other = dot(jnp.where(at == place + 4, 1.0, 0.0).astype(bf16), arrived)
    squares = jnp.sum(own * own + other * other, axis=1, keepdims=True)
    near, far = both_ref[0].astype(f32), both_ref[1].astype(f32)
    token_squares = jnp.sum(near * near + far * far, axis=1, keepdims=True)
    half = token_squares.shape[0] // 2
    token_squares = jnp.where(first, token_squares[:half], token_squares[half:])
    squares = jnp.concatenate([squares, token_squares], axis=0) * (1.0 / D)
    parts = three_parts(to_row(squares, 256))
    line = iota((8, 256), 0)
    extra = jnp.where(line == 0, parts[0], jnp.where(line == 1, parts[1], parts[2]))
    extra = jnp.where(line < 3, extra, 0.0).astype(bf16)
    own = (own * gain_ref[...]).astype(bf16)
    swapped = sent_ref[out_ref.shape[0]].astype(f32)
    gain_other = swapped[0:1] + swapped[1:2] + swapped[2:3]
    other = (other * gain_other).astype(bf16)
    for n in range(out_ref.shape[0]):
        cut = slice(n * 128, (n + 1) * 128)
        part = dot(own, jnp.concatenate([gate_ref[:, cut], up_ref[:, cut]], axis=1)) + dot(
            other, jnp.concatenate([gate_other_ref[:, cut], up_other_ref[:, cut]], axis=1)
        )
        out_ref[n, :slots] = part.astype(bf16)
        out_ref[n, slots : slots + half] = (kept_ref[n] + sent_ref[n].astype(f32)).astype(bf16)
        out_ref[n, slots + half :] = extra


def hidden_kernel(parts_ref, out_ref):
    rows = out_ref.shape[0]
    total = parts_ref[0].astype(f32)
    for n in range(1, parts_ref.shape[0]):
        total = total + parts_ref[n].astype(f32)
    mean = total[rows : rows + 1] + total[rows + 1 : rows + 2] + total[rows + 2 : rows + 3]
    scale = to_column(lax.rsqrt(mean + EPS), rows)
    gate = jnp.where(scale > 0.0, total[:rows, :128] * scale, 0.0)
    up = jnp.where(scale > 0.0, total[:rows, 128:] * scale, 0.0)
    out_ref[...] = (gate / (1.0 + jnp.exp(-gate)) * up).astype(bf16)


def lanes_of(ref, core, lo, hi):
    return jnp.concatenate([ref[n, lo:hi] for n in range(core, ref.shape[0], 2)], axis=1)


def down_kernel(hidden_ref, down_ref, shared_down_ref, out_ref, shared_ref):
    sent = out_ref.shape[0]
    slots = 3 * sent // 8
    down = down_ref[...]
    rows = jnp.concatenate(
        [dot(lanes_of(hidden_ref, core, 0, slots), down).astype(bf16) for core in range(2)], axis=0
    )
    to, at = iota((sent, 2 * slots), 0), iota((sent, 2 * slots), 1)
    place = (to & 7) * (sent // 8) + (to >> 3)
    out_ref[...] = dot(jnp.where(at == place, 1.0, 0.0).astype(bf16), rows).astype(bf16)

    end = hidden_ref.shape[1]
    hidden = jnp.concatenate(
        [lanes_of(hidden_ref, core, slots, end) for core in range(2)], axis=0
    )
    shared_ref[...] = dot(hidden, shared_down_ref[...])


def combine_kernel(rows_ref, weights_ref, shared_ref, gain_ref, mixed_ref, squares_ref):
    rows = rows_ref[...]
    mixed = shared_ref[...]
    for n in range(3):
        mixed = mixed + dot(weights_ref[n], rows)
    mixed_ref[...] = mixed * gain_ref[...]
    squares = to_row(jnp.sum(mixed * mixed, axis=1, keepdims=True), 128)
    squares_ref[...] = jnp.broadcast_to(squares[None], squares_ref.shape)


def norm_kernel(squares_ref, mixed_ref, out_ref):
    total = jnp.sum(squares_ref[...], axis=0)
    scale = to_column(lax.rsqrt(total / D + EPS), out_ref.shape[0])
    out_ref[...] = (mixed_ref[...] * scale).astype(bf16)


def call(body, out, *operands, flops=0):
    def spec(array):
        return pl.BlockSpec(memory_space=pltpu.SMEM if array.shape == (1,) else pltpu.VMEM)

    outs = out if isinstance(out, tuple) else (out,)
    specs = tuple(pl.BlockSpec(memory_space=pltpu.VMEM) for _ in outs)
    moved = sum(a.size * a.dtype.itemsize for a in (*operands, *outs))
    return pl.pallas_call(
        body,
        out_shape=out,
        in_specs=[spec(a) for a in operands],
        out_specs=specs if isinstance(out, tuple) else specs[0],
        compiler_params=pltpu.CompilerParams(vmem_limit_bytes=24 * MIB),
        cost_estimate=pl.CostEstimate(flops=flops, bytes_accessed=moved, transcendentals=0),
    )(*operands)


def shape(dims, dtype):
    return jax.ShapeDtypeStruct(dims, dtype)


def per_device(
    tokens,
    norm_gain,
    routes,
    route_weights,
    gate_proj,
    up_proj,
    down_proj,
    shared_gate,
    shared_up,
    shared_down,
    out_gain,
):
    rows, features = tokens.shape
    sources, lines, cores = (lax.axis_size(a) for a in ("ep", "x", "core"))
    sent = sources * 8
    slots = sources * 3
    half = rows // 2
    core = lax.axis_index("core").astype(i32).reshape(1)
    swap = [(0, 1), (1, 0)]
    gain = norm_gain.reshape(1, features)
    gate, up, down = gate_proj[0], up_proj[0], down_proj[0]

    routes, route_weights = routes.T, route_weights.T
    both = lax.all_gather(tokens, "core", axis=0)
    outgoing = call(pack_kernel, shape((sent, features), bf16), core, routes, both)
    arrived = lax.all_to_all(
        outgoing.reshape(sources, 8, features), "ep", 0, 0, tiled=True
    )
    gate_other = lax.ppermute(gate, "core", swap)
    up_other = lax.ppermute(up, "core", swap)
    kept, given, weights, later_gain = call(
        shared_up_kernel,
        (
            shape((lines, half, 256), f32),
            shape((lines + 1, half, 256), bf16),
            shape((3, rows, sent), bf16),
            shape((1, features), f32),
        ),
        core,
        both,
        gain,
        shared_gate,
        shared_up,
        routes,
        route_weights,
        out_gain.reshape(1, features),
        flops=2 * rows * features * 2048,
    )
    taken = lax.ppermute(given, "core", swap)

    parts = call(
        hidden_parts_kernel,
        shape((lines, slots + half + 8, 256), bf16),
        core,
        arrived.reshape(sent, features),
        both,
        gain,
        gate,
        up,
        gate_other,
        up_other,
        kept,
        taken,
        flops=4 * slots * features * 2048,
    )
    parts = lax.all_to_all(parts, "x", 0, 0, tiled=True)
    hidden = call(hidden_kernel, shape((slots + half, 128), bf16), parts)
    hidden = lax.all_gather(hidden, ("x", "core"), axis=0)
    leaving, shared = call(
        down_kernel,
        (shape((sent, features), bf16), shape((rows, features), f32)),
        hidden,
        down,
        shared_down,
        flops=4 * slots * 1024 * features,
    )
    returned = lax.all_to_all(leaving.reshape(sources, 8, features), "ep", 0, 0, tiled=True)
    mixed, squares = call(
        combine_kernel,
        (shape((rows, features), f32), shape((lines * cores, 1, 128), f32)),
        returned.reshape(sent, features),
        weights,
        shared,
        later_gain,
    )
    squares = lax.all_to_all(squares, ("x", "core"), 0, 0, tiled=True)
    return call(norm_kernel, shape((rows, features), bf16), squares, mixed)


def solution(mesh):
    sources, members = mesh.devices.shape
    inner = Mesh(mesh.devices.reshape(sources, members // 2, 2), ("ep", "x", "core"))
    tp = ("x", "core")
    return jax.shard_map(
        per_device,
        mesh=inner,
        in_specs=(
            P("ep", tp),
            P(tp),
            P("ep", None),
            P("ep", None),
            P("ep", tp, None),
            P("ep", tp, None),
            P("ep", None, tp),
            P(tp, None),
            P(tp, None),
            P(None, tp),
            P(tp),
        ),
        out_specs=P("ep", tp),
        check_vma=False,
    )
```

```python
import jax
import jax.numpy as jnp
from jax import lax
from jax.experimental import pallas as pl
from jax.experimental.pallas import tpu as pltpu
from jax.sharding import Mesh, PartitionSpec as P


D = 4096
EPS = 1e-06
bf16, f32, i32 = jnp.bfloat16, jnp.float32, jnp.int32
MIB = 1024 * 1024


def iota(shape, dim):
    return lax.broadcasted_iota(i32, shape, dim)


def dot(a, b):
    return jnp.dot(a, b, preferred_element_type=f32)


def to_row(column, lanes):
    rows = column.shape[0]
    own = iota((rows, lanes), 0) == iota((rows, lanes), 1)
    return jnp.sum(jnp.where(own, column, 0.0), axis=0, keepdims=True)


def to_column(row, rows):
    lanes = row.shape[1]
    own = iota((rows, lanes), 0) == iota((rows, lanes), 1)
    return jnp.sum(jnp.where(own, row, 0.0), axis=1, keepdims=True)


def three_parts(value):
    high = value.astype(bf16).astype(f32)
    rest = jnp.where(high < jnp.inf, value - high, 0.0)
    middle = rest.astype(bf16).astype(f32)
    return high, middle, rest - middle


def named_slots(routes, lanes):
    rows, picks = routes.shape
    expert = iota((rows, lanes), 1) >> 3
    named = routes[:, 0:1] == expert
    for k in range(1, picks):
        named = named | (routes[:, k : k + 1] == expert)
    earlier = (iota((rows, rows), 1) < iota((rows, rows), 0)).astype(f32).astype(bf16)
    rank = dot(earlier, jnp.where(named, 1.0, 0.0).astype(bf16))
    return named, rank.astype(i32)


def pack_kernel(core_ref, routes_ref, both_ref, out_ref):
    core = core_ref[0]
    lanes = out_ref.shape[0]
    named, rank = named_slots(routes_ref[...].T, lanes)
    lane = iota(named.shape, 1)
    slot = lane & 3
    chosen = named & (rank == 3 * core + slot) & (slot < 3)
    other = (lane & 4) > 0
    picks = jnp.concatenate(
        [
            jnp.where(chosen & ~other, 1.0, 0.0).astype(bf16),
            jnp.where(chosen & other, 1.0, 0.0).astype(bf16),
        ],
        axis=0,
    )
    rows = jnp.concatenate([both_ref[core], both_ref[1 - core]], axis=0)
    out_ref[...] = lax.dot_general(
        picks, rows, (((0,), (0,)), ((), ())), preferred_element_type=f32
    ).astype(bf16)


def combine_weights(routes_ref, weights_ref, out_ref):
    routes, given = routes_ref[...].T, weights_ref[...].T
    lanes = out_ref.shape[2]
    named, rank = named_slots(routes, lanes)
    lane = iota(named.shape, 1)
    weight = jnp.zeros(named.shape, f32)
    for k in range(routes.shape[1]):
        weight = jnp.where(routes[:, k : k + 1] == lane >> 3, given[:, k : k + 1], weight)
    weight = jnp.where(named & (rank == (lane & 7)), weight, 0.0)
    for n, part in enumerate(three_parts(weight)):
        out_ref[n] = part.astype(bf16)


def swap_kernel(
    core_ref,
    both_ref,
    gain_ref,
    gate_ref,
    up_ref,
    shared_gate_ref,
    shared_up_ref,
    routes_ref,
    weights_ref,
    out_gain_ref,
    swap_ref,
    keep_ref,
    combine_ref,
    later_gain_ref,
    own_gain,
    shared_gate,
    shared_up,
    routes,
    weights,
    sems,
):
    depth = gate_ref.shape[0]
    pairs = (
        (routes_ref, routes),
        (weights_ref, weights),
        (gain_ref, own_gain),
        (shared_gate_ref, shared_gate),
        (shared_up_ref, shared_up),
        (out_gain_ref, later_gain_ref),
        (gate_ref, swap_ref.at[:depth]),
        (up_ref, swap_ref.at[depth : 2 * depth]),
    )
    copies = [pltpu.make_async_copy(a, b, sems.at[n]) for n, (a, b) in enumerate(pairs)]
    for copy in copies:
        copy.start()
    core = core_ref[0]
    first = core == 0
    for copy in copies[:3]:
        copy.wait()
    combine_weights(routes, weights, combine_ref)
    gain = own_gain[...]
    rows = (both_ref[core].astype(f32) * gain).astype(bf16)
    half = rows.shape[0] // 2
    parts = three_parts(gain)
    line = iota((8, gain.shape[1]), 0)
    gain = jnp.where(line == 0, parts[0], jnp.where(line == 1, parts[1], parts[2]))
    gain = jnp.where(line < 3, gain, 0.0).astype(bf16)
    swap_ref[2 * depth + 2 * half :] = jnp.concatenate([gain] * 4, axis=1)
    for copy in copies[3:5]:
        copy.wait()
    for n in range(keep_ref.shape[0]):
        cut = slice(n * 128, (n + 1) * 128)
        part = dot(rows, jnp.concatenate([shared_gate[:, cut], shared_up[:, cut]], axis=1))
        keep_ref[n] = jnp.where(first, part[:half], part[half:])
        at, lane = 2 * depth + n // 4 * half, n % 4 * 256
        swap_ref[at : at + half, lane : lane + 256] = jnp.where(
            first, part[half:], part[:half]
        ).astype(bf16)
    for copy in copies[5:]:
        copy.wait()


def hidden_parts_kernel(
    core_ref,
    rows_ref,
    both_ref,
    gain_ref,
    near_ref,
    far_ref,
    kept_ref,
    out_ref,
):
    first = core_ref[0] == 0
    arrived = rows_ref[...]
    slots = 3 * arrived.shape[0] // 8
    sources = arrived.shape[0] // 8
    to, at = iota((slots, arrived.shape[0]), 0), iota((slots, arrived.shape[0]), 1)
    place = (to % sources) * 8 + to // sources
    own = dot(jnp.where(at == place, 1.0, 0.0).astype(bf16), arrived)
    other = dot(jnp.where(at == place + 4, 1.0, 0.0).astype(bf16), arrived)
    squares = jnp.sum(own * own + other * other, axis=1, keepdims=True)
    low, high = both_ref[0].astype(f32), both_ref[1].astype(f32)
    token_squares = jnp.sum(low * low + high * high, axis=1, keepdims=True)
    half = token_squares.shape[0] // 2
    token_squares = jnp.where(first, token_squares[:half], token_squares[half:])
    squares = jnp.concatenate([squares, token_squares], axis=0) * (1.0 / D)
    parts = three_parts(to_row(squares, 256))
    line = iota((8, 256), 0)
    extra = jnp.where(line == 0, parts[0], jnp.where(line == 1, parts[1], parts[2]))
    extra = jnp.where(line < 3, extra, 0.0).astype(bf16)
    own = (own * gain_ref[...]).astype(bf16)
    depth = gain_ref.shape[1]
    shared_at = 2 * depth
    swapped = far_ref[shared_at + 2 * half :, :depth].astype(f32)
    gain_other = swapped[0:1] + swapped[1:2] + swapped[2:3]
    other = (other * gain_other).astype(bf16)
    for n in range(out_ref.shape[0]):
        cut = slice(n * 128, (n + 1) * 128)
        near = jnp.concatenate([near_ref[:depth, cut], near_ref[depth:shared_at, cut]], axis=1)
        far = jnp.concatenate([far_ref[:depth, cut], far_ref[depth:shared_at, cut]], axis=1)
        out_ref[n, :slots] = (dot(own, near) + dot(other, far)).astype(bf16)
        at, lane = shared_at + n // 4 * half, n % 4 * 256
        given = far_ref[at : at + half, lane : lane + 256].astype(f32)
        out_ref[n, slots : slots + half] = (kept_ref[n] + given).astype(bf16)
        out_ref[n, slots + half :] = extra


def hidden_kernel(parts_ref, out_ref):
    rows = out_ref.shape[0]
    total = parts_ref[0].astype(f32)
    for n in range(1, parts_ref.shape[0]):
        total = total + parts_ref[n].astype(f32)
    mean = total[rows : rows + 1] + total[rows + 1 : rows + 2] + total[rows + 2 : rows + 3]
    scale = to_column(lax.rsqrt(mean + EPS), rows)
    gate = jnp.where(scale > 0.0, total[:rows, :128] * scale, 0.0)
    up = jnp.where(scale > 0.0, total[:rows, 128:] * scale, 0.0)
    out_ref[...] = (gate / (1.0 + jnp.exp(-gate)) * up).astype(bf16)


def lanes_of(ref, core, lo, hi):
    return jnp.concatenate([ref[n, lo:hi] for n in range(core, ref.shape[0], 2)], axis=1)


def down_kernel(hidden_ref, down_ref, shared_down_ref, out_ref, shared_ref):
    sent = out_ref.shape[0]
    slots = 3 * sent // 8
    down = down_ref[...]
    rows = jnp.concatenate(
        [dot(lanes_of(hidden_ref, core, 0, slots), down).astype(bf16) for core in range(2)], axis=0
    )
    to, at = iota((sent, 2 * slots), 0), iota((sent, 2 * slots), 1)
    place = (to & 7) * (sent // 8) + (to >> 3)
    out_ref[...] = dot(jnp.where(at == place, 1.0, 0.0).astype(bf16), rows).astype(bf16)

    end = hidden_ref.shape[1]
    hidden = jnp.concatenate(
        [lanes_of(hidden_ref, core, slots, end) for core in range(2)], axis=0
    )
    shared_ref[...] = dot(hidden, shared_down_ref[...])


def combine_kernel(rows_ref, weights_ref, shared_ref, gain_ref, mixed_ref, squares_ref):
    rows = rows_ref[...]
    mixed = shared_ref[...]
    for n in range(3):
        mixed = mixed + dot(weights_ref[n], rows)
    mixed_ref[...] = mixed * gain_ref[...]
    squares = to_row(jnp.sum(mixed * mixed, axis=1, keepdims=True), 128)
    squares_ref[...] = jnp.broadcast_to(squares[None], squares_ref.shape)


def norm_kernel(squares_ref, mixed_ref, out_ref):
    total = jnp.sum(squares_ref[...], axis=0)
    scale = to_column(lax.rsqrt(total / D + EPS), out_ref.shape[0])
    out_ref[...] = (mixed_ref[...] * scale).astype(bf16)


def call(body, out, *operands, flops=0, far=(), scratch=()):
    def spec(n, array):
        if n in far:
            return pl.BlockSpec(memory_space=pltpu.HBM)
        return pl.BlockSpec(memory_space=pltpu.SMEM if array.shape == (1,) else pltpu.VMEM)

    operands = [
        pltpu.with_memory_space_constraint(a, pltpu.HBM) if n in far else a
        for n, a in enumerate(operands)
    ]
    outs = out if isinstance(out, tuple) else (out,)
    specs = tuple(pl.BlockSpec(memory_space=pltpu.VMEM) for _ in outs)
    moved = sum(a.size * a.dtype.itemsize for a in (*operands, *outs))
    return pl.pallas_call(
        body,
        out_shape=out,
        in_specs=[spec(n, a) for n, a in enumerate(operands)],
        out_specs=specs if isinstance(out, tuple) else specs[0],
        scratch_shapes=scratch,
        compiler_params=pltpu.CompilerParams(vmem_limit_bytes=24 * MIB),
        cost_estimate=pl.CostEstimate(flops=flops, bytes_accessed=moved, transcendentals=0),
    )(*operands)


def shape(dims, dtype):
    return jax.ShapeDtypeStruct(dims, dtype)


def per_device(
    tokens,
    norm_gain,
    routes,
    route_weights,
    gate_proj,
    up_proj,
    down_proj,
    shared_gate,
    shared_up,
    shared_down,
    out_gain,
):
    rows, features = tokens.shape
    sources, lines, cores = (lax.axis_size(a) for a in ("ep", "x", "core"))
    sent = sources * 8
    slots = sources * 3
    half = rows // 2
    core = lax.axis_index("core").astype(i32).reshape(1)
    swap = [(0, 1), (1, 0)]
    gain = norm_gain.reshape(1, features)
    gate, up, down = gate_proj[0], up_proj[0], down_proj[0]

    routes, route_weights = routes.T, route_weights.T
    both = lax.all_gather(tokens, "core", axis=0)
    outgoing = call(pack_kernel, shape((sent, features), bf16), core, routes, both)
    arrived = lax.all_to_all(
        outgoing.reshape(sources, 8, features), "ep", 0, 0, tiled=True
    )
    near, kept, weights, later_gain = call(
        swap_kernel,
        (
            shape((2 * features + 2 * half + 8, 1024), bf16),
            shape((lines, half, 256), f32),
            shape((3, rows, sent), bf16),
            shape((1, features), f32),
        ),
        core,
        both,
        gain,
        gate,
        up,
        shared_gate,
        shared_up,
        routes,
        route_weights,
        out_gain.reshape(1, features),
        flops=2 * rows * features * 2048,
        far=range(2, 10),
        scratch=[
            pltpu.VMEM((1, features), f32),
            pltpu.VMEM((features, 1024), bf16),
            pltpu.VMEM((features, 1024), bf16),
            pltpu.VMEM(routes.shape, i32),
            pltpu.VMEM(route_weights.shape, f32),
            pltpu.SemaphoreType.DMA((8,)),
        ],
    )
    far = lax.ppermute(near, "core", swap)

    parts = call(
        hidden_parts_kernel,
        shape((lines, slots + half + 8, 256), bf16),
        core,
        arrived.reshape(sent, features),
        both,
        gain,
        near,
        far,
        kept,
        flops=4 * slots * features * 2048,
    )
    parts = lax.all_to_all(parts, "x", 0, 0, tiled=True)
    hidden = call(hidden_kernel, shape((slots + half, 128), bf16), parts)
    hidden = lax.all_gather(hidden, ("x", "core"), axis=0)
    leaving, shared = call(
        down_kernel,
        (shape((sent, features), bf16), shape((rows, features), f32)),
        hidden,
        down,
        shared_down,
        flops=4 * slots * 1024 * features,
    )
    returned = lax.all_to_all(leaving.reshape(sources, 8, features), "ep", 0, 0, tiled=True)
    mixed, squares = call(
        combine_kernel,
        (shape((rows, features), f32), shape((lines * cores, 1, 128), f32)),
        returned.reshape(sent, features),
        weights,
        shared,
        later_gain,
    )
    squares = lax.all_to_all(squares, ("x", "core"), 0, 0, tiled=True)
    return call(norm_kernel, shape((rows, features), bf16), squares, mixed)


def solution(mesh):
    sources, members = mesh.devices.shape
    inner = Mesh(mesh.devices.reshape(sources, members // 2, 2), ("ep", "x", "core"))
    tp = ("x", "core")
    return jax.shard_map(
        per_device,
        mesh=inner,
        in_specs=(
            P("ep", tp),
            P(tp),
            P("ep", None),
            P("ep", None),
            P("ep", tp, None),
            P("ep", tp, None),
            P("ep", None, tp),
            P(tp, None),
            P(tp, None),
            P(None, tp),
            P(tp),
        ),
        out_specs=P("ep", tp),
        check_vma=False,
    )
```

```python
import jax
import jax.numpy as jnp
from jax import lax
from jax.experimental import pallas as pl
from jax.experimental.pallas import tpu as pltpu
from jax.sharding import Mesh, PartitionSpec as P


D = 4096
EPS = 1e-06
bf16, f32, i32 = jnp.bfloat16, jnp.float32, jnp.int32
MIB = 1024 * 1024


def iota(shape, dim):
    return lax.broadcasted_iota(i32, shape, dim)


def dot(a, b):
    return jnp.dot(a, b, preferred_element_type=f32)


def to_row(column, lanes):
    rows = column.shape[0]
    own = iota((rows, lanes), 0) == iota((rows, lanes), 1)
    return jnp.sum(jnp.where(own, column, 0.0), axis=0, keepdims=True)


def to_column(row, rows):
    lanes = row.shape[1]
    own = iota((rows, lanes), 0) == iota((rows, lanes), 1)
    return jnp.sum(jnp.where(own, row, 0.0), axis=1, keepdims=True)


def three_parts(value):
    high = value.astype(bf16).astype(f32)
    rest = jnp.where(high < jnp.inf, value - high, 0.0)
    middle = rest.astype(bf16).astype(f32)
    return high, middle, rest - middle


def named_slots(routes, lanes):
    rows, picks = routes.shape
    lane = iota((rows, lanes), 1)
    expert = (lane * 43691) >> 19
    named = routes[:, 0:1] == expert
    for k in range(1, picks):
        named = named | (routes[:, k : k + 1] == expert)
    earlier = (iota((rows, rows), 1) < iota((rows, rows), 0)).astype(f32).astype(bf16)
    rank = dot(earlier, jnp.where(named, 1.0, 0.0).astype(bf16))
    return named, rank.astype(i32), expert, lane - 12 * expert


def quarters(core, both_ref):
    own, other = both_ref[core], both_ref[1 - core]
    return own[:, :128], own[:, 128:], other[:, :128], other[:, 128:]


def pack_kernel(core_ref, routes_ref, both_ref, out_ref):
    core = core_ref[0]
    named, rank, _, line = named_slots(routes_ref[...].T, out_ref.shape[0])
    chosen = jnp.where(named & (rank == 3 * core + (line >> 2)), 1.0, 0.0)
    picks = jnp.concatenate(
        [jnp.where((line & 3) == q, chosen, 0.0).astype(bf16) for q in range(4)], axis=0
    )
    rows = jnp.concatenate(quarters(core, both_ref), axis=0)
    out_ref[...] = lax.dot_general(
        picks, rows, (((0,), (0,)), ((), ())), preferred_element_type=f32
    ).astype(bf16)


def combine_weights(routes_ref, weights_ref, out_ref):
    routes, given = routes_ref[...].T, weights_ref[...].T
    named, rank, expert, line = named_slots(routes, out_ref.shape[1])
    weight = jnp.zeros(named.shape, f32)
    for k in range(routes.shape[1]):
        weight = jnp.where(routes[:, k : k + 1] == expert, given[:, k : k + 1], weight)
    slot = 3 * ((line >> 1) & 1) + (line >> 2)
    weight = jnp.where(named & (rank == slot), weight, 0.0)
    rows = weight.shape[0]
    at = 0
    for part in three_parts(weight):
        for side in range(2):
            out_ref[at : at + rows] = jnp.where((line & 1) == side, part, 0.0).astype(bf16)
            at += rows


def swap_kernel(
    core_ref,
    both_ref,
    gain_ref,
    gate_ref,
    up_ref,
    shared_gate_ref,
    shared_up_ref,
    routes_ref,
    weights_ref,
    out_gain_ref,
    swap_ref,
    keep_ref,
    combine_ref,
    later_gain_ref,
    own_gain,
    shared_gate,
    shared_up,
    routes,
    weights,
    sems,
):
    depth = gate_ref.shape[0]
    pairs = (
        (routes_ref, routes),
        (weights_ref, weights),
        (gain_ref, own_gain),
        (shared_gate_ref, shared_gate),
        (shared_up_ref, shared_up),
        (out_gain_ref, later_gain_ref),
        (gate_ref, swap_ref.at[:depth]),
        (up_ref, swap_ref.at[depth : 2 * depth]),
    )
    copies = [pltpu.make_async_copy(a, b, sems.at[n]) for n, (a, b) in enumerate(pairs)]
    for copy in copies:
        copy.start()
    core = core_ref[0]
    first = core == 0
    for copy in copies[:3]:
        copy.wait()
    combine_weights(routes, weights, combine_ref)
    gain = own_gain[...]
    rows = (both_ref[core].astype(f32) * gain).astype(bf16)
    half = rows.shape[0] // 2
    parts = three_parts(gain)
    line = iota((8, gain.shape[1]), 0)
    gain = jnp.where(line == 0, parts[0], jnp.where(line == 1, parts[1], parts[2]))
    gain = jnp.where(line < 3, gain, 0.0).astype(bf16)
    swap_ref[2 * depth + 2 * half :] = jnp.concatenate([gain] * 4, axis=1)
    for copy in copies[3:5]:
        copy.wait()
    for n in range(keep_ref.shape[0]):
        cut = slice(n * 128, (n + 1) * 128)
        part = dot(rows, jnp.concatenate([shared_gate[:, cut], shared_up[:, cut]], axis=1))
        keep_ref[n] = jnp.where(first, part[:half], part[half:])
        at, lane = 2 * depth + n // 4 * half, n % 4 * 256
        swap_ref[at : at + half, lane : lane + 256] = jnp.where(
            first, part[half:], part[:half]
        ).astype(bf16)
    for copy in copies[5:]:
        copy.wait()


def hidden_parts_kernel(
    core_ref,
    rows_ref,
    both_ref,
    gain_ref,
    near_ref,
    far_ref,
    kept_ref,
    out_ref,
    wide,
):
    first = core_ref[0] == 0
    slots = rows_ref.shape[0] // 4
    wide[...] = rows_ref[...].astype(f32)
    own, other = (
        jnp.concatenate([wide[pl.ds(q, slots, stride=4), :] for q in pair], axis=1)
        for pair in ((0, 1), (2, 3))
    )
    squares = jnp.sum(own * own + other * other, axis=1, keepdims=True)
    low, high = both_ref[0].astype(f32), both_ref[1].astype(f32)
    token_squares = jnp.sum(low * low + high * high, axis=1, keepdims=True)
    half = token_squares.shape[0] // 2
    token_squares = jnp.where(first, token_squares[:half], token_squares[half:])
    squares = jnp.concatenate([squares, token_squares], axis=0) * (1.0 / D)
    parts = three_parts(to_row(squares, 256))
    line = iota((8, 256), 0)
    extra = jnp.where(line == 0, parts[0], jnp.where(line == 1, parts[1], parts[2]))
    extra = jnp.where(line < 3, extra, 0.0).astype(bf16)
    own = (own * gain_ref[...]).astype(bf16)
    depth = gain_ref.shape[1]
    shared_at = 2 * depth
    swapped = far_ref[shared_at + 2 * half :, :depth].astype(f32)
    gain_other = swapped[0:1] + swapped[1:2] + swapped[2:3]
    other = (other * gain_other).astype(bf16)
    for n in range(out_ref.shape[0]):
        cut = slice(n * 128, (n + 1) * 128)
        near = jnp.concatenate([near_ref[:depth, cut], near_ref[depth:shared_at, cut]], axis=1)
        far = jnp.concatenate([far_ref[:depth, cut], far_ref[depth:shared_at, cut]], axis=1)
        out_ref[n, :slots] = (dot(own, near) + dot(other, far)).astype(bf16)
        at, lane = shared_at + n // 4 * half, n % 4 * 256
        given = far_ref[at : at + half, lane : lane + 256].astype(f32)
        out_ref[n, slots : slots + half] = (kept_ref[n] + given).astype(bf16)
        out_ref[n, slots + half :] = extra


def hidden_kernel(parts_ref, out_ref):
    rows = out_ref.shape[0]
    total = parts_ref[0].astype(f32)
    for n in range(1, parts_ref.shape[0]):
        total = total + parts_ref[n].astype(f32)
    mean = total[rows : rows + 1] + total[rows + 1 : rows + 2] + total[rows + 2 : rows + 3]
    scale = to_column(lax.rsqrt(mean + EPS), rows)
    gate = jnp.where(scale > 0.0, total[:rows, :128] * scale, 0.0)
    up = jnp.where(scale > 0.0, total[:rows, 128:] * scale, 0.0)
    out_ref[...] = (gate / (1.0 + jnp.exp(-gate)) * up).astype(bf16)


def lanes_of(ref, core, lo, hi):
    return jnp.concatenate([ref[n, lo:hi] for n in range(core, ref.shape[0], 2)], axis=1)


def down_kernel(hidden_ref, down_ref, shared_down_ref, out_ref, shared_ref, wide):
    slots = out_ref.shape[0] // 4
    down = down_ref[...]
    for core in range(2):
        rows = dot(lanes_of(hidden_ref, core, 0, slots), down)
        for side in range(2):
            wide[pl.ds(2 * core + side, slots, stride=4), :] = rows[
                :, side * 128 : (side + 1) * 128
            ]
    out_ref[...] = wide[...].astype(bf16)
    end = hidden_ref.shape[1]
    hidden = jnp.concatenate(
        [lanes_of(hidden_ref, core, slots, end) for core in range(2)], axis=0
    )
    shared_ref[...] = dot(hidden, shared_down_ref[...])


def combine_kernel(rows_ref, weights_ref, shared_ref, gain_ref, mixed_ref, squares_ref):
    parts = dot(weights_ref[...], rows_ref[...])
    count = shared_ref.shape[0]
    low, high = (
        sum(parts[at * count : (at + 1) * count] for at in (side, side + 2, side + 4))
        for side in range(2)
    )
    mixed = shared_ref[...] + jnp.concatenate([low, high], axis=1)
    mixed_ref[...] = mixed * gain_ref[...]
    squares = to_row(jnp.sum(mixed * mixed, axis=1, keepdims=True), 128)
    squares_ref[...] = jnp.broadcast_to(squares[None], squares_ref.shape)


def norm_kernel(squares_ref, mixed_ref, out_ref):
    total = jnp.sum(squares_ref[...], axis=0)
    scale = to_column(lax.rsqrt(total / D + EPS), out_ref.shape[0])
    out_ref[...] = (mixed_ref[...] * scale).astype(bf16)


def call(body, out, *operands, flops=0, far=(), scratch=()):
    def spec(n, array):
        if n in far:
            return pl.BlockSpec(memory_space=pltpu.HBM)
        return pl.BlockSpec(memory_space=pltpu.SMEM if array.shape == (1,) else pltpu.VMEM)

    operands = [
        pltpu.with_memory_space_constraint(a, pltpu.HBM) if n in far else a
        for n, a in enumerate(operands)
    ]
    outs = out if isinstance(out, tuple) else (out,)
    specs = tuple(pl.BlockSpec(memory_space=pltpu.VMEM) for _ in outs)
    moved = sum(a.size * a.dtype.itemsize for a in (*operands, *outs))
    return pl.pallas_call(
        body,
        out_shape=out,
        in_specs=[spec(n, a) for n, a in enumerate(operands)],
        out_specs=specs if isinstance(out, tuple) else specs[0],
        scratch_shapes=scratch,
        compiler_params=pltpu.CompilerParams(vmem_limit_bytes=24 * MIB),
        cost_estimate=pl.CostEstimate(flops=flops, bytes_accessed=moved, transcendentals=0),
    )(*operands)


def shape(dims, dtype):
    return jax.ShapeDtypeStruct(dims, dtype)


def exchanged(rows, sources):
    blocks = rows.reshape(sources, -1, 4, 128)
    return lax.all_to_all(blocks, "ep", 0, 0, tiled=True).reshape(rows.shape)


def per_device(
    tokens,
    norm_gain,
    routes,
    route_weights,
    gate_proj,
    up_proj,
    down_proj,
    shared_gate,
    shared_up,
    shared_down,
    out_gain,
):
    rows, features = tokens.shape
    sources, lines, cores = (lax.axis_size(a) for a in ("ep", "x", "core"))
    sent = sources * 12
    slots = sources * 3
    half = rows // 2
    core = lax.axis_index("core").astype(i32).reshape(1)
    swap = [(0, 1), (1, 0)]
    gain = norm_gain.reshape(1, features)
    gate, up, down = gate_proj[0], up_proj[0], down_proj[0]

    routes, route_weights = routes.T, route_weights.T
    both = lax.all_gather(tokens, "core", axis=0)
    outgoing = call(pack_kernel, shape((sent, 128), bf16), core, routes, both)
    arrived = exchanged(outgoing, sources)
    near, kept, weights, later_gain = call(
        swap_kernel,
        (
            shape((2 * features + 2 * half + 8, 1024), bf16),
            shape((lines, half, 256), f32),
            shape((6 * rows, sent), bf16),
            shape((1, features), f32),
        ),
        core,
        both,
        gain,
        gate,
        up,
        shared_gate,
        shared_up,
        routes,
        route_weights,
        out_gain.reshape(1, features),
        flops=2 * rows * features * 2048,
        far=range(2, 10),
        scratch=[
            pltpu.VMEM((1, features), f32),
            pltpu.VMEM((features, 1024), bf16),
            pltpu.VMEM((features, 1024), bf16),
            pltpu.VMEM(routes.shape, i32),
            pltpu.VMEM(route_weights.shape, f32),
            pltpu.SemaphoreType.DMA((8,)),
        ],
    )
    far = lax.ppermute(near, "core", swap)

    parts = call(
        hidden_parts_kernel,
        shape((lines, slots + half + 8, 256), bf16),
        core,
        arrived,
        both,
        gain,
        near,
        far,
        kept,
        flops=4 * slots * features * 2048,
        scratch=[pltpu.VMEM((sent, 128), f32)],
    )
    parts = lax.all_to_all(parts, "x", 0, 0, tiled=True)
    hidden = call(hidden_kernel, shape((slots + half, 128), bf16), parts)
    hidden = lax.all_gather(hidden, ("x", "core"), axis=0)
    leaving, shared = call(
        down_kernel,
        (shape((sent, 128), bf16), shape((rows, features), f32)),
        hidden,
        down,
        shared_down,
        scratch=[pltpu.VMEM((sent, 128), f32)],
        flops=4 * slots * 1024 * features,
    )
    returned = exchanged(leaving, sources)
    mixed, squares = call(
        combine_kernel,
        (shape((rows, features), f32), shape((lines * cores, 1, 128), f32)),
        returned,
        weights,
        shared,
        later_gain,
    )
    squares = lax.all_to_all(squares, ("x", "core"), 0, 0, tiled=True)
    return call(norm_kernel, shape((rows, features), bf16), squares, mixed)


def solution(mesh):
    sources, members = mesh.devices.shape
    inner = Mesh(mesh.devices.reshape(sources, members // 2, 2), ("ep", "x", "core"))
    tp = ("x", "core")
    return jax.shard_map(
        per_device,
        mesh=inner,
        in_specs=(
            P("ep", tp),
            P(tp),
            P("ep", None),
            P("ep", None),
            P("ep", tp, None),
            P("ep", tp, None),
            P("ep", None, tp),
            P(tp, None),
            P(tp, None),
            P(None, tp),
            P(tp),
        ),
        out_specs=P("ep", tp),
        check_vma=False,
    )
```

```python
import jax
import jax.numpy as jnp
from jax import lax
from jax.experimental import pallas as pl
from jax.experimental.pallas import tpu as pltpu
from jax.sharding import Mesh, PartitionSpec as P


D = 4096
EPS = 1e-06
bf16, f32, i32 = jnp.bfloat16, jnp.float32, jnp.int32
MIB = 1024 * 1024


def iota(shape, dim):
    return lax.broadcasted_iota(i32, shape, dim)


def dot(a, b):
    return jnp.dot(a, b, preferred_element_type=f32)


def to_row(column, lanes):
    rows = column.shape[0]
    own = iota((rows, lanes), 0) == iota((rows, lanes), 1)
    return jnp.sum(jnp.where(own, column, 0.0), axis=0, keepdims=True)


def to_column(row, rows):
    lanes = row.shape[1]
    own = iota((rows, lanes), 0) == iota((rows, lanes), 1)
    return jnp.sum(jnp.where(own, row, 0.0), axis=1, keepdims=True)


def three_parts(value):
    high = value.astype(bf16).astype(f32)
    rest = jnp.where(high < jnp.inf, value - high, 0.0)
    middle = rest.astype(bf16).astype(f32)
    return high, middle, rest - middle


def named_slots(routes, lanes):
    rows, picks = routes.shape
    lane = iota((rows, lanes), 1)
    expert = (lane * 43691) >> 19
    named = routes[:, 0:1] == expert
    for k in range(1, picks):
        named = named | (routes[:, k : k + 1] == expert)
    earlier = (iota((rows, rows), 1) < iota((rows, rows), 0)).astype(f32).astype(bf16)
    rank = dot(earlier, jnp.where(named, 1.0, 0.0).astype(bf16))
    return named, rank.astype(i32), expert, lane - 12 * expert


def quarters(core, both_ref):
    own, other = both_ref[core], both_ref[1 - core]
    return own[:, :128], own[:, 128:], other[:, :128], other[:, 128:]


def pack_kernel(core_ref, routes_ref, both_ref, out_ref):
    core = core_ref[0]
    named, rank, _, line = named_slots(routes_ref[...].T, out_ref.shape[0])
    chosen = jnp.where(named & (rank == 3 * core + (line >> 2)), 1.0, 0.0)
    picks = jnp.concatenate(
        [jnp.where((line & 3) == q, chosen, 0.0).astype(bf16) for q in range(4)], axis=0
    )
    rows = jnp.concatenate(quarters(core, both_ref), axis=0)
    out_ref[...] = lax.dot_general(
        picks, rows, (((0,), (0,)), ((), ())), preferred_element_type=f32
    ).astype(bf16)


def combine_weights(core, routes_ref, weights_ref, out_ref):
    routes, given = routes_ref[...].T, weights_ref[...].T
    named, rank, expert, line = named_slots(routes, out_ref.shape[1])
    weight = jnp.zeros(named.shape, f32)
    for k in range(routes.shape[1]):
        weight = jnp.where(routes[:, k : k + 1] == expert, given[:, k : k + 1], weight)
    weight = jnp.where(named & (rank == 3 * core + (line >> 2)), weight, 0.0)
    rows = weight.shape[0]
    at = 0
    for part in three_parts(weight):
        for quarter in range(4):
            out_ref[at : at + rows] = jnp.where((line & 3) == quarter, part, 0.0).astype(bf16)
            at += rows


def swap_kernel(
    core_ref,
    both_ref,
    gain_ref,
    gate_ref,
    up_ref,
    shared_gate_ref,
    shared_up_ref,
    routes_ref,
    weights_ref,
    out_gain_ref,
    swap_ref,
    combine_ref,
    later_gain_ref,
    own_gain,
    shared_gate,
    shared_up,
    routes,
    weights,
    sems,
):
    depth = gate_ref.shape[0]
    pairs = (
        (routes_ref, routes),
        (weights_ref, weights),
        (gain_ref, own_gain),
        (shared_gate_ref, shared_gate),
        (shared_up_ref, shared_up),
        (out_gain_ref, later_gain_ref),
        (gate_ref, swap_ref.at[:depth]),
        (up_ref, swap_ref.at[depth : 2 * depth]),
    )
    copies = [pltpu.make_async_copy(a, b, sems.at[n]) for n, (a, b) in enumerate(pairs)]
    for copy in copies:
        copy.start()
    core = core_ref[0]
    first = core == 0
    for copy in copies[:3]:
        copy.wait()
    combine_weights(core, routes, weights, combine_ref)
    gain = own_gain[...]
    rows = (both_ref[core].astype(f32) * gain).astype(bf16)
    half = rows.shape[0] // 2
    parts = three_parts(gain)
    line = iota((8, gain.shape[1]), 0)
    gain = jnp.where(line == 0, parts[0], jnp.where(line == 1, parts[1], parts[2]))
    gain = jnp.where(line < 3, gain, 0.0).astype(bf16)
    gain_at = 2 * depth + 2 * half
    kept_at = gain_at + 8
    swap_ref[gain_at:kept_at] = jnp.concatenate([gain] * 4, axis=1)
    for copy in copies[3:5]:
        copy.wait()
    for n in range(8):
        cut = slice(n * 128, (n + 1) * 128)
        part = dot(rows, jnp.concatenate([shared_gate[:, cut], shared_up[:, cut]], axis=1))
        low, high = part[:half].astype(bf16), part[half:].astype(bf16)
        lanes = slice(n % 4 * 256, n % 4 * 256 + 256)
        at = n // 4 * half
        swap_ref[2 * depth + at : 2 * depth + at + half, lanes] = jnp.where(first, high, low)
        swap_ref[kept_at + at : kept_at + at + half, lanes] = jnp.where(first, low, high)
    for copy in copies[5:]:
        copy.wait()


def hidden_parts_kernel(
    core_ref,
    rows_ref,
    both_ref,
    gain_ref,
    near_ref,
    far_ref,
    out_ref,
    wide,
):
    first = core_ref[0] == 0
    slots = rows_ref.shape[0] // 4
    wide[...] = rows_ref[...].astype(f32)
    own, other = (
        jnp.concatenate([wide[pl.ds(q, slots, stride=4), :] for q in pair], axis=1)
        for pair in ((0, 1), (2, 3))
    )
    squares = jnp.sum(own * own + other * other, axis=1, keepdims=True)
    low, high = both_ref[0].astype(f32), both_ref[1].astype(f32)
    token_squares = jnp.sum(low * low + high * high, axis=1, keepdims=True)
    half = token_squares.shape[0] // 2
    token_squares = jnp.where(first, token_squares[:half], token_squares[half:])
    squares = jnp.concatenate([squares, token_squares], axis=0) * (1.0 / D)
    parts = three_parts(to_row(squares, 256))
    line = iota((8, 256), 0)
    extra = jnp.where(line == 0, parts[0], jnp.where(line == 1, parts[1], parts[2]))
    extra = jnp.where(line < 3, extra, 0.0).astype(bf16)
    own = (own * gain_ref[...]).astype(bf16)
    depth = gain_ref.shape[1]
    shared_at = 2 * depth
    kept_at = shared_at + 2 * half + 8
    swapped = far_ref[kept_at - 8 : kept_at, :depth].astype(f32)
    gain_other = swapped[0:1] + swapped[1:2] + swapped[2:3]
    other = (other * gain_other).astype(bf16)
    for n in range(out_ref.shape[0]):
        cut = slice(n * 128, (n + 1) * 128)
        near = jnp.concatenate([near_ref[:depth, cut], near_ref[depth:shared_at, cut]], axis=1)
        far = jnp.concatenate([far_ref[:depth, cut], far_ref[depth:shared_at, cut]], axis=1)
        out_ref[n, :slots] = (dot(own, near) + dot(other, far)).astype(bf16)
        at, lanes = n // 4 * half, slice(n % 4 * 256, n % 4 * 256 + 256)
        given = far_ref[shared_at + at : shared_at + at + half, lanes].astype(f32)
        kept = near_ref[kept_at + at : kept_at + at + half, lanes].astype(f32)
        out_ref[n, slots : slots + half] = (kept + given).astype(bf16)
        out_ref[n, slots + half :] = extra


def hidden_kernel(parts_ref, out_ref):
    rows = out_ref.shape[1]
    total = parts_ref[0].astype(f32)
    for n in range(1, parts_ref.shape[0]):
        total = total + parts_ref[n].astype(f32)
    mean = total[rows : rows + 1] + total[rows + 1 : rows + 2] + total[rows + 2 : rows + 3]
    scale = to_column(lax.rsqrt(mean + EPS), rows)
    gate = jnp.where(scale > 0.0, total[:rows, :128] * scale, 0.0)
    up = jnp.where(scale > 0.0, total[:rows, 128:] * scale, 0.0)
    hidden = (gate / (1.0 + jnp.exp(-gate)) * up).astype(bf16)
    for n in range(out_ref.shape[0]):
        out_ref[n] = hidden


def down_kernel(
    hidden_ref, near_ref, far_ref, near_shared_ref, far_shared_ref, out_ref, shared_ref, wide
):
    slots = out_ref.shape[0] // 4
    hidden = jnp.concatenate([hidden_ref[n] for n in range(hidden_ref.shape[0])], axis=1)
    shared_refs = (near_shared_ref, far_shared_ref)
    for n, down_ref in enumerate((near_ref, far_ref)):
        rows = dot(hidden[:slots], down_ref[...])
        for side in range(2):
            wide[pl.ds(2 * n + side, slots, stride=4), :] = rows[
                :, side * 128 : (side + 1) * 128
            ]
        shared_ref[n] = dot(hidden[slots:], shared_refs[n][...])
    out_ref[...] = wide[...].astype(bf16)


def combine_kernel(core_ref, rows_ref, weights_ref, shared_ref, near_ref, far_ref):
    first = core_ref[0] == 0
    parts = dot(weights_ref[...], rows_ref[...])
    count = near_ref.shape[0]
    quarter = [
        sum(parts[at * count : (at + 1) * count] for at in (n, n + 4, n + 8)) for n in range(4)
    ]
    for n, out_ref in enumerate((near_ref, far_ref)):
        shared = shared_ref[n]
        none = jnp.zeros_like(shared)
        low, high = jnp.where(first, shared, none), jnp.where(first, none, shared)
        out_ref[...] = jnp.concatenate(quarter[2 * n : 2 * n + 2], axis=1) + jnp.concatenate(
            [low, high], axis=0
        )


def mix_kernel(core_ref, near_ref, both_ref, gain_ref, mixed_ref, squares_ref):
    mixed = near_ref[...] + both_ref[1 - core_ref[0]]
    mixed_ref[...] = mixed * gain_ref[...]
    squares = to_row(jnp.sum(mixed * mixed, axis=1, keepdims=True), 128)
    squares_ref[...] = jnp.broadcast_to(squares[None], squares_ref.shape)


def norm_kernel(squares_ref, mixed_ref, out_ref):
    total = jnp.sum(squares_ref[...], axis=0)
    scale = to_column(lax.rsqrt(total / D + EPS), out_ref.shape[0])
    out_ref[...] = (mixed_ref[...] * scale).astype(bf16)


def call(body, out, *operands, flops=0, far=(), scratch=()):
    def spec(n, array):
        if n in far:
            return pl.BlockSpec(memory_space=pltpu.HBM)
        return pl.BlockSpec(memory_space=pltpu.SMEM if array.shape == (1,) else pltpu.VMEM)

    operands = [
        pltpu.with_memory_space_constraint(a, pltpu.HBM) if n in far else a
        for n, a in enumerate(operands)
    ]
    outs = out if isinstance(out, tuple) else (out,)
    specs = tuple(pl.BlockSpec(memory_space=pltpu.VMEM) for _ in outs)
    moved = sum(a.size * a.dtype.itemsize for a in (*operands, *outs))
    return pl.pallas_call(
        body,
        out_shape=out,
        in_specs=[spec(n, a) for n, a in enumerate(operands)],
        out_specs=specs if isinstance(out, tuple) else specs[0],
        scratch_shapes=scratch,
        compiler_params=pltpu.CompilerParams(vmem_limit_bytes=24 * MIB),
        cost_estimate=pl.CostEstimate(flops=flops, bytes_accessed=moved, transcendentals=0),
    )(*operands)


def shape(dims, dtype):
    return jax.ShapeDtypeStruct(dims, dtype)


def exchanged(rows, sources):
    blocks = rows.reshape(sources, -1, 4, 128)
    return lax.all_to_all(blocks, "ep", 0, 0, tiled=True).reshape(rows.shape)


def per_device(
    tokens,
    norm_gain,
    routes,
    route_weights,
    gate_proj,
    up_proj,
    down_proj,
    shared_gate,
    shared_up,
    shared_down,
    out_gain,
):
    rows, features = tokens.shape
    sources, lines, cores = (lax.axis_size(a) for a in ("ep", "x", "core"))
    sent = sources * 12
    slots = sources * 3
    half = rows // 2
    core = lax.axis_index("core").astype(i32).reshape(1)
    swap = [(0, 1), (1, 0)]
    gain = norm_gain.reshape(1, features)
    gate, up, down = gate_proj[0], up_proj[0], down_proj[0]

    routes, route_weights = routes.T, route_weights.T
    both = lax.all_gather(tokens, "core", axis=0)
    outgoing = call(pack_kernel, shape((sent, 128), bf16), core, routes, both)
    arrived = exchanged(outgoing, sources)
    near, weights, later_gain = call(
        swap_kernel,
        (
            shape((2 * features + 4 * half + 8, 1024), bf16),
            shape((12 * rows, sent), bf16),
            shape((1, features), f32),
        ),
        core,
        both,
        gain,
        gate,
        up,
        shared_gate,
        shared_up,
        routes,
        route_weights,
        out_gain.reshape(1, features),
        flops=2 * rows * features * 2048,
        far=range(2, 10),
        scratch=[
            pltpu.VMEM((1, features), f32),
            pltpu.VMEM((features, 1024), bf16),
            pltpu.VMEM((features, 1024), bf16),
            pltpu.VMEM(routes.shape, i32),
            pltpu.VMEM(route_weights.shape, f32),
            pltpu.SemaphoreType.DMA((8,)),
        ],
    )
    far = lax.ppermute(near, "core", swap)
    far_down = lax.ppermute(down, "core", swap)
    far_shared = lax.ppermute(shared_down, "core", swap)
    far, far_down, far_shared = lax.optimization_barrier((far, far_down, far_shared))

    parts = call(
        hidden_parts_kernel,
        shape((lines, slots + half + 8, 256), bf16),
        core,
        arrived,
        both,
        gain,
        near,
        far,
        flops=4 * slots * features * 2048,
        scratch=[pltpu.VMEM((sent, 128), f32)],
    )
    parts = lax.all_to_all(parts, "x", 0, 0, tiled=True)
    hidden = call(hidden_kernel, shape((lines, slots + half, 128), bf16), parts)
    hidden = lax.all_to_all(hidden, "x", 0, 0, tiled=True)
    leaving, shared = call(
        down_kernel,
        (shape((sent, 128), bf16), shape((2, half, features), f32)),
        hidden,
        down,
        far_down,
        shared_down,
        far_shared,
        scratch=[pltpu.VMEM((sent, 128), f32)],
        flops=4 * slots * 1024 * features,
    )
    returned = exchanged(leaving, sources)
    near_mixed, far_mixed = call(
        combine_kernel,
        (shape((rows, features), f32), shape((rows, features), f32)),
        core,
        returned,
        weights,
        shared,
    )
    far_mixed = lax.all_gather(far_mixed, "core", axis=0)
    mixed, squares = call(
        mix_kernel,
        (shape((rows, features), f32), shape((lines * cores, 1, 128), f32)),
        core,
        near_mixed,
        far_mixed,
        later_gain,
    )
    squares = lax.all_to_all(squares, ("x", "core"), 0, 0, tiled=True)
    return call(norm_kernel, shape((rows, features), bf16), squares, mixed)


def solution(mesh):
    sources, members = mesh.devices.shape
    inner = Mesh(mesh.devices.reshape(sources, members // 2, 2), ("ep", "x", "core"))
    tp = ("x", "core")
    return jax.shard_map(
        per_device,
        mesh=inner,
        in_specs=(
            P("ep", tp),
            P(tp),
            P("ep", None),
            P("ep", None),
            P("ep", tp, None),
            P("ep", tp, None),
            P("ep", None, tp),
            P(tp, None),
            P(tp, None),
            P(None, tp),
            P(tp),
        ),
        out_specs=P("ep", tp),
        check_vma=False,
    )
```

```python
import jax
import jax.numpy as jnp
from jax import lax
from jax.experimental import pallas as pl
from jax.experimental.pallas import tpu as pltpu
from jax.sharding import Mesh, PartitionSpec as P


D = 4096
EPS = 1e-06
bf16, f32, i32 = jnp.bfloat16, jnp.float32, jnp.int32
MIB = 1024 * 1024


def iota(shape, dim):
    return lax.broadcasted_iota(i32, shape, dim)


def dot(a, b):
    return jnp.dot(a, b, preferred_element_type=f32)


def to_row(column, lanes):
    rows = column.shape[0]
    own = iota((rows, lanes), 0) == iota((rows, lanes), 1)
    return jnp.sum(jnp.where(own, column, 0.0), axis=0, keepdims=True)


def to_column(row, rows):
    lanes = row.shape[1]
    own = iota((rows, lanes), 0) == iota((rows, lanes), 1)
    return jnp.sum(jnp.where(own, row, 0.0), axis=1, keepdims=True)


def three_parts(value):
    high = value.astype(bf16).astype(f32)
    rest = jnp.where(high < jnp.inf, value - high, 0.0)
    middle = rest.astype(bf16).astype(f32)
    return high, middle, rest - middle


def named_slots(routes, lanes):
    rows, picks = routes.shape
    lane = iota((rows, lanes), 1)
    expert = (lane * 43691) >> 19
    named = routes[:, 0:1] == expert
    for k in range(1, picks):
        named = named | (routes[:, k : k + 1] == expert)
    earlier = (iota((rows, rows), 1) < iota((rows, rows), 0)).astype(f32).astype(bf16)
    rank = dot(earlier, jnp.where(named, 1.0, 0.0).astype(bf16))
    return named, rank.astype(i32), expert, lane - 12 * expert


def quarters(core, both_ref):
    own, other = both_ref[core], both_ref[1 - core]
    return own[:, :128], own[:, 128:], other[:, :128], other[:, 128:]


def pack_kernel(core_ref, routes_ref, both_ref, out_ref):
    core = core_ref[0]
    named, rank, _, line = named_slots(routes_ref[...].T, out_ref.shape[0])
    chosen = jnp.where(named & (rank == 3 * core + (line >> 2)), 1.0, 0.0)
    picks = jnp.concatenate(
        [jnp.where((line & 3) == q, chosen, 0.0).astype(bf16) for q in range(4)], axis=0
    )
    rows = jnp.concatenate(quarters(core, both_ref), axis=0)
    out_ref[...] = lax.dot_general(
        picks, rows, (((0,), (0,)), ((), ())), preferred_element_type=f32
    ).astype(bf16)


def combine_weights(routes_ref, weights_ref, out_ref):
    routes, given = routes_ref[...].T, weights_ref[...].T
    named, rank, expert, line = named_slots(routes, out_ref.shape[1])
    weight = jnp.zeros(named.shape, f32)
    for k in range(routes.shape[1]):
        weight = jnp.where(routes[:, k : k + 1] == expert, given[:, k : k + 1], weight)
    slot = 3 * ((line >> 1) & 1) + (line >> 2)
    weight = jnp.where(named & (rank == slot), weight, 0.0)
    rows = weight.shape[0]
    at = 0
    for part in three_parts(weight):
        for side in range(2):
            out_ref[at : at + rows] = jnp.where((line & 1) == side, part, 0.0).astype(bf16)
            at += rows


def swap_kernel(
    core_ref,
    both_ref,
    gain_ref,
    gate_ref,
    up_ref,
    shared_gate_ref,
    shared_up_ref,
    routes_ref,
    weights_ref,
    out_gain_ref,
    swap_ref,
    keep_ref,
    combine_ref,
    later_gain_ref,
    own_gain,
    shared_gate,
    shared_up,
    routes,
    weights,
    sems,
):
    depth = gate_ref.shape[0]
    pairs = (
        (routes_ref, routes),
        (weights_ref, weights),
        (gain_ref, own_gain),
        (shared_gate_ref, shared_gate),
        (shared_up_ref, shared_up),
        (out_gain_ref, later_gain_ref),
        (gate_ref, swap_ref.at[:depth]),
        (up_ref, swap_ref.at[depth : 2 * depth]),
    )
    copies = [pltpu.make_async_copy(a, b, sems.at[n]) for n, (a, b) in enumerate(pairs)]
    for copy in copies:
        copy.start()
    core = core_ref[0]
    first = core == 0
    for copy in copies[:3]:
        copy.wait()
    combine_weights(routes, weights, combine_ref)
    gain = own_gain[...]
    rows = (both_ref[core].astype(f32) * gain).astype(bf16)
    half = rows.shape[0] // 2
    parts = three_parts(gain)
    line = iota((8, gain.shape[1]), 0)
    gain = jnp.where(line == 0, parts[0], jnp.where(line == 1, parts[1], parts[2]))
    gain = jnp.where(line < 3, gain, 0.0).astype(bf16)
    swap_ref[2 * depth + 2 * half :] = jnp.concatenate([gain] * 4, axis=1)
    for copy in copies[3:5]:
        copy.wait()
    for n in range(keep_ref.shape[0]):
        cut = slice(n * 128, (n + 1) * 128)
        part = dot(rows, jnp.concatenate([shared_gate[:, cut], shared_up[:, cut]], axis=1))
        keep_ref[n] = jnp.where(first, part[:half], part[half:])
        at, lane = 2 * depth + n // 4 * half, n % 4 * 256
        swap_ref[at : at + half, lane : lane + 256] = jnp.where(
            first, part[half:], part[:half]
        ).astype(bf16)
    for copy in copies[5:]:
        copy.wait()


def hidden_parts_kernel(
    core_ref,
    rows_ref,
    both_ref,
    gain_ref,
    near_ref,
    far_ref,
    kept_ref,
    out_ref,
    wide,
):
    first = core_ref[0] == 0
    slots = rows_ref.shape[0] // 4
    wide[...] = rows_ref[...].astype(f32)
    own, other = (
        jnp.concatenate([wide[pl.ds(q, slots, stride=4), :] for q in pair], axis=1)
        for pair in ((0, 1), (2, 3))
    )
    squares = jnp.sum(own * own + other * other, axis=1, keepdims=True)
    low, high = both_ref[0].astype(f32), both_ref[1].astype(f32)
    token_squares = jnp.sum(low * low + high * high, axis=1, keepdims=True)
    half = token_squares.shape[0] // 2
    token_squares = jnp.where(first, token_squares[:half], token_squares[half:])
    squares = jnp.concatenate([squares, token_squares], axis=0) * (1.0 / D)
    parts = three_parts(to_row(squares, 256))
    line = iota((8, 256), 0)
    extra = jnp.where(line == 0, parts[0], jnp.where(line == 1, parts[1], parts[2]))
    extra = jnp.where(line < 3, extra, 0.0).astype(bf16)
    own = (own * gain_ref[...]).astype(bf16)
    depth = gain_ref.shape[1]
    shared_at = 2 * depth
    swapped = far_ref[shared_at + 2 * half :, :depth].astype(f32)
    gain_other = swapped[0:1] + swapped[1:2] + swapped[2:3]
    other = (other * gain_other).astype(bf16)
    for n in range(out_ref.shape[0]):
        cut = slice(n * 128, (n + 1) * 128)
        near = jnp.concatenate([near_ref[:depth, cut], near_ref[depth:shared_at, cut]], axis=1)
        far = jnp.concatenate([far_ref[:depth, cut], far_ref[depth:shared_at, cut]], axis=1)
        out_ref[n, :slots] = (dot(own, near) + dot(other, far)).astype(bf16)
        at, lane = shared_at + n // 4 * half, n % 4 * 256
        given = far_ref[at : at + half, lane : lane + 256].astype(f32)
        out_ref[n, slots : slots + half] = (kept_ref[n] + given).astype(bf16)
        out_ref[n, slots + half :] = extra


def hidden_kernel(parts_ref, out_ref):
    rows = out_ref.shape[1]
    total = parts_ref[0].astype(f32)
    for n in range(1, parts_ref.shape[0]):
        total = total + parts_ref[n].astype(f32)
    mean = total[rows : rows + 1] + total[rows + 1 : rows + 2] + total[rows + 2 : rows + 3]
    scale = to_column(lax.rsqrt(mean + EPS), rows)
    gate = jnp.where(scale > 0.0, total[:rows, :128] * scale, 0.0)
    up = jnp.where(scale > 0.0, total[:rows, 128:] * scale, 0.0)
    hidden = (gate / (1.0 + jnp.exp(-gate)) * up).astype(bf16)
    for n in range(out_ref.shape[0]):
        out_ref[n] = hidden


def lanes_of(ref, core, lo, hi):
    return jnp.concatenate([ref[core, n, lo:hi] for n in range(ref.shape[1])], axis=1)


def down_kernel(hidden_ref, down_ref, shared_down_ref, out_ref, shared_ref, wide):
    slots = out_ref.shape[0] // 4
    down = down_ref[...]
    for core in range(2):
        rows = dot(lanes_of(hidden_ref, core, 0, slots), down)
        for side in range(2):
            wide[pl.ds(2 * core + side, slots, stride=4), :] = rows[
                :, side * 128 : (side + 1) * 128
            ]
    out_ref[...] = wide[...].astype(bf16)
    end = hidden_ref.shape[2]
    hidden = jnp.concatenate(
        [lanes_of(hidden_ref, core, slots, end) for core in range(2)], axis=0
    )
    shared_ref[...] = dot(hidden, shared_down_ref[...])


def combine_kernel(rows_ref, weights_ref, shared_ref, gain_ref, mixed_ref, squares_ref):
    parts = dot(weights_ref[...], rows_ref[...])
    count = shared_ref.shape[0]
    low, high = (
        sum(parts[at * count : (at + 1) * count] for at in (side, side + 2, side + 4))
        for side in range(2)
    )
    mixed = shared_ref[...] + jnp.concatenate([low, high], axis=1)
    mixed_ref[...] = mixed * gain_ref[...]
    squares = to_row(jnp.sum(mixed * mixed, axis=1, keepdims=True), 128)
    squares_ref[...] = jnp.broadcast_to(squares[None], squares_ref.shape)


def norm_kernel(squares_ref, mixed_ref, out_ref):
    total = jnp.sum(squares_ref[...], axis=0)
    scale = to_column(lax.rsqrt(total / D + EPS), out_ref.shape[0])
    out_ref[...] = (mixed_ref[...] * scale).astype(bf16)


def call(body, out, *operands, flops=0, far=(), scratch=()):
    def spec(n, array):
        if n in far:
            return pl.BlockSpec(memory_space=pltpu.HBM)
        return pl.BlockSpec(memory_space=pltpu.SMEM if array.shape == (1,) else pltpu.VMEM)

    operands = [
        pltpu.with_memory_space_constraint(a, pltpu.HBM) if n in far else a
        for n, a in enumerate(operands)
    ]
    outs = out if isinstance(out, tuple) else (out,)
    specs = tuple(pl.BlockSpec(memory_space=pltpu.VMEM) for _ in outs)
    moved = sum(a.size * a.dtype.itemsize for a in (*operands, *outs))
    return pl.pallas_call(
        body,
        out_shape=out,
        in_specs=[spec(n, a) for n, a in enumerate(operands)],
        out_specs=specs if isinstance(out, tuple) else specs[0],
        scratch_shapes=scratch,
        compiler_params=pltpu.CompilerParams(vmem_limit_bytes=24 * MIB),
        cost_estimate=pl.CostEstimate(flops=flops, bytes_accessed=moved, transcendentals=0),
    )(*operands)


def shape(dims, dtype):
    return jax.ShapeDtypeStruct(dims, dtype)


def exchanged(rows, sources):
    blocks = rows.reshape(sources, -1, 4, 128)
    return lax.all_to_all(blocks, "ep", 0, 0, tiled=True).reshape(rows.shape)


def per_device(
    tokens,
    norm_gain,
    routes,
    route_weights,
    gate_proj,
    up_proj,
    down_proj,
    shared_gate,
    shared_up,
    shared_down,
    out_gain,
):
    rows, features = tokens.shape
    sources, lines, cores = (lax.axis_size(a) for a in ("ep", "x", "core"))
    sent = sources * 12
    slots = sources * 3
    half = rows // 2
    core = lax.axis_index("core").astype(i32).reshape(1)
    swap = [(0, 1), (1, 0)]
    gain = norm_gain.reshape(1, features)
    gate, up, down = gate_proj[0], up_proj[0], down_proj[0]

    routes, route_weights = routes.T, route_weights.T
    both = lax.all_gather(tokens, "core", axis=0)
    outgoing = call(pack_kernel, shape((sent, 128), bf16), core, routes, both)
    arrived = exchanged(outgoing, sources)
    near, kept, weights, later_gain = call(
        swap_kernel,
        (
            shape((2 * features + 2 * half + 8, 1024), bf16),
            shape((lines, half, 256), f32),
            shape((6 * rows, sent), bf16),
            shape((1, features), f32),
        ),
        core,
        both,
        gain,
        gate,
        up,
        shared_gate,
        shared_up,
        routes,
        route_weights,
        out_gain.reshape(1, features),
        flops=2 * rows * features * 2048,
        far=range(2, 10),
        scratch=[
            pltpu.VMEM((1, features), f32),
            pltpu.VMEM((features, 1024), bf16),
            pltpu.VMEM((features, 1024), bf16),
            pltpu.VMEM(routes.shape, i32),
            pltpu.VMEM(route_weights.shape, f32),
            pltpu.SemaphoreType.DMA((8,)),
        ],
    )
    far = lax.ppermute(near, "core", swap)

    parts = call(
        hidden_parts_kernel,
        shape((lines, slots + half + 8, 256), bf16),
        core,
        arrived,
        both,
        gain,
        near,
        far,
        kept,
        flops=4 * slots * features * 2048,
        scratch=[pltpu.VMEM((sent, 128), f32)],
    )
    parts = lax.all_to_all(parts, "x", 0, 0, tiled=True)
    hidden = call(hidden_kernel, shape((lines, slots + half, 128), bf16), parts)
    hidden = lax.all_to_all(hidden, "x", 0, 0, tiled=True)
    hidden = lax.all_gather(hidden, "core", axis=0)
    leaving, shared = call(
        down_kernel,
        (shape((sent, 128), bf16), shape((rows, features), f32)),
        hidden,
        down,
        shared_down,
        scratch=[pltpu.VMEM((sent, 128), f32)],
        flops=4 * slots * 1024 * features,
    )
    returned = exchanged(leaving, sources)
    mixed, squares = call(
        combine_kernel,
        (shape((rows, features), f32), shape((lines * cores, 1, 128), f32)),
        returned,
        weights,
        shared,
        later_gain,
    )
    squares = lax.all_to_all(squares, ("x", "core"), 0, 0, tiled=True)
    return call(norm_kernel, shape((rows, features), bf16), squares, mixed)


def solution(mesh):
    sources, members = mesh.devices.shape
    inner = Mesh(mesh.devices.reshape(sources, members // 2, 2), ("ep", "x", "core"))
    tp = ("x", "core")
    return jax.shard_map(
        per_device,
        mesh=inner,
        in_specs=(
            P("ep", tp),
            P(tp),
            P("ep", None),
            P("ep", None),
            P("ep", tp, None),
            P("ep", tp, None),
            P("ep", None, tp),
            P(tp, None),
            P(tp, None),
            P(None, tp),
            P(tp),
        ),
        out_specs=P("ep", tp),
        check_vma=False,
    )
```

```python
import jax
import jax.numpy as jnp
from jax import lax
from jax.experimental import pallas as pl
from jax.experimental.pallas import tpu as pltpu
from jax.sharding import Mesh, PartitionSpec as P


D = 4096
EPS = 1e-06
bf16, f32, i32 = jnp.bfloat16, jnp.float32, jnp.int32
MIB = 1024 * 1024


def iota(shape, dim):
    return lax.broadcasted_iota(i32, shape, dim)


def dot(a, b):
    return jnp.dot(a, b, preferred_element_type=f32)


def to_row(column, lanes):
    rows = column.shape[0]
    own = iota((rows, lanes), 0) == iota((rows, lanes), 1)
    return jnp.sum(jnp.where(own, column, 0.0), axis=0, keepdims=True)


def to_column(row, rows):
    lanes = row.shape[1]
    own = iota((rows, lanes), 0) == iota((rows, lanes), 1)
    return jnp.sum(jnp.where(own, row, 0.0), axis=1, keepdims=True)


def three_parts(value):
    high = value.astype(bf16).astype(f32)
    rest = jnp.where(high < jnp.inf, value - high, 0.0)
    middle = rest.astype(bf16).astype(f32)
    return high, middle, rest - middle


def named_slots(routes, lanes):
    rows, picks = routes.shape
    lane = iota((rows, lanes), 1)
    expert = (lane * 43691) >> 19
    named = routes[:, 0:1] == expert
    for k in range(1, picks):
        named = named | (routes[:, k : k + 1] == expert)
    earlier = (iota((rows, rows), 1) < iota((rows, rows), 0)).astype(f32).astype(bf16)
    rank = dot(earlier, jnp.where(named, 1.0, 0.0).astype(bf16))
    return named, rank.astype(i32), expert, lane - 12 * expert


def quarters(core, both_ref):
    own, other = both_ref[core], both_ref[1 - core]
    return own[:, :128], own[:, 128:], other[:, :128], other[:, 128:]


def pack_kernel(core_ref, routes_ref, both_ref, out_ref, routes, sem):
    copy = pltpu.make_async_copy(routes_ref, routes, sem)
    copy.start()
    core = core_ref[0]
    copy.wait()
    named, rank, _, line = named_slots(routes[...].T, out_ref.shape[0])
    chosen = jnp.where(named & (rank == 3 * core + (line >> 2)), 1.0, 0.0)
    picks = jnp.concatenate(
        [jnp.where((line & 3) == q, chosen, 0.0).astype(bf16) for q in range(4)], axis=0
    )
    rows = jnp.concatenate(quarters(core, both_ref), axis=0)
    out_ref[...] = lax.dot_general(
        picks, rows, (((0,), (0,)), ((), ())), preferred_element_type=f32
    ).astype(bf16)


def combine_weights(routes_ref, weights_ref, out_ref):
    routes, given = routes_ref[...].T, weights_ref[...].T
    named, rank, expert, line = named_slots(routes, out_ref.shape[1])
    weight = jnp.zeros(named.shape, f32)
    for k in range(routes.shape[1]):
        weight = jnp.where(routes[:, k : k + 1] == expert, given[:, k : k + 1], weight)
    slot = 3 * ((line >> 1) & 1) + (line >> 2)
    weight = jnp.where(named & (rank == slot), weight, 0.0)
    rows = weight.shape[0]
    at = 0
    for part in three_parts(weight):
        for side in range(2):
            out_ref[at : at + rows] = jnp.where((line & 1) == side, part, 0.0).astype(bf16)
            at += rows


def swap_kernel(
    core_ref,
    both_ref,
    gain_ref,
    gate_ref,
    up_ref,
    shared_gate_ref,
    shared_up_ref,
    routes_ref,
    weights_ref,
    out_gain_ref,
    swap_ref,
    keep_ref,
    combine_ref,
    later_gain_ref,
    own_gain,
    shared_gate,
    shared_up,
    routes,
    weights,
    sems,
):
    depth = gate_ref.shape[0]
    pairs = (
        (routes_ref, routes),
        (weights_ref, weights),
        (gain_ref, own_gain),
        (shared_gate_ref, shared_gate),
        (shared_up_ref, shared_up),
        (out_gain_ref, later_gain_ref),
        (gate_ref, swap_ref.at[:depth]),
        (up_ref, swap_ref.at[depth : 2 * depth]),
    )
    copies = [pltpu.make_async_copy(a, b, sems.at[n]) for n, (a, b) in enumerate(pairs)]
    for copy in copies:
        copy.start()
    core = core_ref[0]
    first = core == 0
    for copy in copies[:3]:
        copy.wait()
    combine_weights(routes, weights, combine_ref)
    gain = own_gain[...]
    rows = (both_ref[core].astype(f32) * gain).astype(bf16)
    half = rows.shape[0] // 2
    parts = three_parts(gain)
    line = iota((8, gain.shape[1]), 0)
    gain = jnp.where(line == 0, parts[0], jnp.where(line == 1, parts[1], parts[2]))
    gain = jnp.where(line < 3, gain, 0.0).astype(bf16)
    swap_ref[2 * depth + 2 * half :] = jnp.concatenate([gain] * 4, axis=1)
    for copy in copies[3:5]:
        copy.wait()
    for n in range(keep_ref.shape[0]):
        cut = slice(n * 128, (n + 1) * 128)
        part = dot(rows, jnp.concatenate([shared_gate[:, cut], shared_up[:, cut]], axis=1))
        keep_ref[n] = jnp.where(first, part[:half], part[half:])
        at, lane = 2 * depth + n // 4 * half, n % 4 * 256
        swap_ref[at : at + half, lane : lane + 256] = jnp.where(
            first, part[half:], part[:half]
        ).astype(bf16)
    for copy in copies[5:]:
        copy.wait()


def hidden_parts_kernel(
    core_ref,
    rows_ref,
    both_ref,
    gain_ref,
    near_ref,
    far_ref,
    kept_ref,
    out_ref,
    wide,
):
    first = core_ref[0] == 0
    slots = rows_ref.shape[0] // 4
    wide[...] = rows_ref[...].astype(f32)
    own, other = (
        jnp.concatenate([wide[pl.ds(q, slots, stride=4), :] for q in pair], axis=1)
        for pair in ((0, 1), (2, 3))
    )
    squares = jnp.sum(own * own + other * other, axis=1, keepdims=True)
    low, high = both_ref[0].astype(f32), both_ref[1].astype(f32)
    token_squares = jnp.sum(low * low + high * high, axis=1, keepdims=True)
    half = token_squares.shape[0] // 2
    token_squares = jnp.where(first, token_squares[:half], token_squares[half:])
    squares = jnp.concatenate([squares, token_squares], axis=0) * (1.0 / D)
    parts = three_parts(to_row(squares, 256))
    line = iota((8, 256), 0)
    extra = jnp.where(line == 0, parts[0], jnp.where(line == 1, parts[1], parts[2]))
    extra = jnp.where(line < 3, extra, 0.0).astype(bf16)
    own = (own * gain_ref[...]).astype(bf16)
    depth = gain_ref.shape[1]
    shared_at = 2 * depth
    swapped = far_ref[shared_at + 2 * half :, :depth].astype(f32)
    gain_other = swapped[0:1] + swapped[1:2] + swapped[2:3]
    other = (other * gain_other).astype(bf16)
    for n in range(out_ref.shape[0]):
        cut = slice(n * 128, (n + 1) * 128)
        near = jnp.concatenate([near_ref[:depth, cut], near_ref[depth:shared_at, cut]], axis=1)
        far = jnp.concatenate([far_ref[:depth, cut], far_ref[depth:shared_at, cut]], axis=1)
        out_ref[n, :slots] = (dot(own, near) + dot(other, far)).astype(bf16)
        at, lane = shared_at + n // 4 * half, n % 4 * 256
        given = far_ref[at : at + half, lane : lane + 256].astype(f32)
        out_ref[n, slots : slots + half] = (kept_ref[n] + given).astype(bf16)
        out_ref[n, slots + half :] = extra


def hidden_kernel(parts_ref, out_ref):
    rows = out_ref.shape[0]
    total = parts_ref[0].astype(f32)
    for n in range(1, parts_ref.shape[0]):
        total = total + parts_ref[n].astype(f32)
    mean = total[rows : rows + 1] + total[rows + 1 : rows + 2] + total[rows + 2 : rows + 3]
    scale = to_column(lax.rsqrt(mean + EPS), rows)
    gate = jnp.where(scale > 0.0, total[:rows, :128] * scale, 0.0)
    up = jnp.where(scale > 0.0, total[:rows, 128:] * scale, 0.0)
    out_ref[...] = (gate / (1.0 + jnp.exp(-gate)) * up).astype(bf16)


def lanes_of(ref, core, lo, hi):
    return jnp.concatenate([ref[n, lo:hi] for n in range(core, ref.shape[0], 2)], axis=1)


def down_kernel(hidden_ref, down_ref, shared_down_ref, out_ref, shared_ref, wide):
    slots = out_ref.shape[0] // 4
    down = down_ref[...]
    for core in range(2):
        rows = dot(lanes_of(hidden_ref, core, 0, slots), down)
        for side in range(2):
            wide[pl.ds(2 * core + side, slots, stride=4), :] = rows[
                :, side * 128 : (side + 1) * 128
            ]
    out_ref[...] = wide[...].astype(bf16)
    end = hidden_ref.shape[1]
    hidden = jnp.concatenate(
        [lanes_of(hidden_ref, core, slots, end) for core in range(2)], axis=0
    )
    shared_ref[...] = dot(hidden, shared_down_ref[...])


def combine_kernel(rows_ref, weights_ref, shared_ref, mixed_ref, squares_ref):
    parts = dot(weights_ref[...], rows_ref[...])
    count = shared_ref.shape[0]
    low, high = (
        sum(parts[at * count : (at + 1) * count] for at in (side, side + 2, side + 4))
        for side in range(2)
    )
    mixed = shared_ref[...] + jnp.concatenate([low, high], axis=1)
    mixed_ref[...] = mixed
    squares = to_row(jnp.sum(mixed * mixed, axis=1, keepdims=True), 128)
    squares_ref[...] = jnp.broadcast_to(squares[None], squares_ref.shape)


def norm_kernel(squares_ref, mixed_ref, gain_ref, out_ref):
    total = jnp.sum(squares_ref[...], axis=0)
    scale = to_column(lax.rsqrt(total / D + EPS), out_ref.shape[0])
    out_ref[...] = (mixed_ref[...] * scale * gain_ref[...]).astype(bf16)


def call(body, out, *operands, flops=0, far=(), scratch=()):
    def spec(n, array):
        if n in far:
            return pl.BlockSpec(memory_space=pltpu.HBM)
        return pl.BlockSpec(memory_space=pltpu.SMEM if array.shape == (1,) else pltpu.VMEM)

    operands = [
        pltpu.with_memory_space_constraint(a, pltpu.HBM) if n in far else a
        for n, a in enumerate(operands)
    ]
    outs = out if isinstance(out, tuple) else (out,)
    specs = tuple(pl.BlockSpec(memory_space=pltpu.VMEM) for _ in outs)
    moved = sum(a.size * a.dtype.itemsize for a in (*operands, *outs))
    return pl.pallas_call(
        body,
        out_shape=out,
        in_specs=[spec(n, a) for n, a in enumerate(operands)],
        out_specs=specs if isinstance(out, tuple) else specs[0],
        scratch_shapes=scratch,
        compiler_params=pltpu.CompilerParams(vmem_limit_bytes=24 * MIB),
        cost_estimate=pl.CostEstimate(flops=flops, bytes_accessed=moved, transcendentals=0),
    )(*operands)


def shape(dims, dtype):
    return jax.ShapeDtypeStruct(dims, dtype)


def exchanged(rows, sources):
    blocks = rows.reshape(sources, -1, 4, 128)
    return lax.all_to_all(blocks, "ep", 0, 0, tiled=True).reshape(rows.shape)


def per_device(
    tokens,
    norm_gain,
    routes,
    route_weights,
    gate_proj,
    up_proj,
    down_proj,
    shared_gate,
    shared_up,
    shared_down,
    out_gain,
):
    rows, features = tokens.shape
    sources, lines, cores = (lax.axis_size(a) for a in ("ep", "x", "core"))
    sent = sources * 12
    slots = sources * 3
    half = rows // 2
    core = lax.axis_index("core").astype(i32).reshape(1)
    swap = [(0, 1), (1, 0)]
    gain = norm_gain.reshape(1, features)
    gate, up, down = gate_proj[0], up_proj[0], down_proj[0]

    routes, route_weights = routes.T, route_weights.T
    both = lax.all_gather(tokens, "core", axis=0)
    outgoing = call(
        pack_kernel,
        shape((sent, 128), bf16),
        core,
        routes,
        both,
        far=(1,),
        scratch=[pltpu.VMEM(routes.shape, i32), pltpu.SemaphoreType.DMA],
    )
    arrived = exchanged(outgoing, sources)
    near, kept, weights, later_gain = call(
        swap_kernel,
        (
            shape((2 * features + 2 * half + 8, 1024), bf16),
            shape((lines, half, 256), f32),
            shape((6 * rows, sent), bf16),
            shape((1, features), f32),
        ),
        core,
        both,
        gain,
        gate,
        up,
        shared_gate,
        shared_up,
        routes,
        route_weights,
        out_gain.reshape(1, features),
        flops=2 * rows * features * 2048,
        far=range(2, 10),
        scratch=[
            pltpu.VMEM((1, features), f32),
            pltpu.VMEM((features, 1024), bf16),
            pltpu.VMEM((features, 1024), bf16),
            pltpu.VMEM(routes.shape, i32),
            pltpu.VMEM(route_weights.shape, f32),
            pltpu.SemaphoreType.DMA((8,)),
        ],
    )
    far = lax.ppermute(near, "core", swap)

    parts = call(
        hidden_parts_kernel,
        shape((lines, slots + half + 8, 256), bf16),
        core,
        arrived,
        both,
        gain,
        near,
        far,
        kept,
        flops=4 * slots * features * 2048,
        scratch=[pltpu.VMEM((sent, 128), f32)],
    )
    parts = lax.all_to_all(parts, "x", 0, 0, tiled=True)
    hidden = call(hidden_kernel, shape((slots + half, 128), bf16), parts)
    hidden = lax.all_gather(hidden, ("x", "core"), axis=0)
    leaving, shared = call(
        down_kernel,
        (shape((sent, 128), bf16), shape((rows, features), f32)),
        hidden,
        down,
        shared_down,
        scratch=[pltpu.VMEM((sent, 128), f32)],
        flops=4 * slots * 1024 * features,
    )
    returned = exchanged(leaving, sources)
    mixed, squares = call(
        combine_kernel,
        (shape((rows, features), f32), shape((lines * cores, 1, 128), f32)),
        returned,
        weights,
        shared,
    )
    squares = lax.all_to_all(squares, ("x", "core"), 0, 0, tiled=True)
    return call(norm_kernel, shape((rows, features), bf16), squares, mixed, later_gain)


def solution(mesh):
    sources, members = mesh.devices.shape
    inner = Mesh(mesh.devices.reshape(sources, members // 2, 2), ("ep", "x", "core"))
    tp = ("x", "core")
    return jax.shard_map(
        per_device,
        mesh=inner,
        in_specs=(
            P("ep", tp),
            P(tp),
            P("ep", None),
            P("ep", None),
            P("ep", tp, None),
            P("ep", tp, None),
            P("ep", None, tp),
            P(tp, None),
            P(tp, None),
            P(None, tp),
            P(tp),
        ),
        out_specs=P("ep", tp),
        check_vma=False,
    )
```

```python
import jax
import jax.numpy as jnp
from jax import lax
from jax.experimental import pallas as pl
from jax.experimental.pallas import tpu as pltpu
from jax.sharding import Mesh, PartitionSpec as P


D = 4096
EPS = 1e-06
bf16, f32, i32 = jnp.bfloat16, jnp.float32, jnp.int32
MIB = 1024 * 1024


def iota(shape, dim):
    return lax.broadcasted_iota(i32, shape, dim)


def dot(a, b):
    return jnp.dot(a, b, preferred_element_type=f32)


def to_row(column, lanes):
    rows = column.shape[0]
    own = iota((rows, lanes), 0) == iota((rows, lanes), 1)
    return jnp.sum(jnp.where(own, column, 0.0), axis=0, keepdims=True)


def to_column(row, rows):
    lanes = row.shape[1]
    own = iota((rows, lanes), 0) == iota((rows, lanes), 1)
    return jnp.sum(jnp.where(own, row, 0.0), axis=1, keepdims=True)


def three_parts(value):
    high = value.astype(bf16).astype(f32)
    rest = jnp.where(high < jnp.inf, value - high, 0.0)
    middle = rest.astype(bf16).astype(f32)
    return high, middle, rest - middle


def named_slots(routes, lanes):
    rows, picks = routes.shape
    lane = iota((rows, lanes), 1)
    expert = (lane * 43691) >> 19
    named = routes[:, 0:1] == expert
    for k in range(1, picks):
        named = named | (routes[:, k : k + 1] == expert)
    earlier = (iota((rows, rows), 1) < iota((rows, rows), 0)).astype(f32).astype(bf16)
    rank = dot(earlier, jnp.where(named, 1.0, 0.0).astype(bf16))
    return named, rank.astype(i32), expert, lane - 12 * expert


def quarters(core, both_ref):
    own, other = both_ref[core], both_ref[1 - core]
    return own[:, :128], own[:, 128:], other[:, :128], other[:, 128:]


def packed(core, routes, both_ref, lanes):
    named, rank, _, line = named_slots(routes, lanes)
    chosen = jnp.where(named & (rank == 3 * core + (line >> 2)), 1.0, 0.0)
    picks = jnp.concatenate(
        [jnp.where((line & 3) == q, chosen, 0.0).astype(bf16) for q in range(4)], axis=0
    )
    rows = jnp.concatenate(quarters(core, both_ref), axis=0)
    return lax.dot_general(
        picks, rows, (((0,), (0,)), ((), ())), preferred_element_type=f32
    ).astype(bf16)


def combine_weights(routes_ref, weights_ref, out_ref):
    routes, given = routes_ref[...].T, weights_ref[...].T
    named, rank, expert, line = named_slots(routes, out_ref.shape[1])
    weight = jnp.zeros(named.shape, f32)
    for k in range(routes.shape[1]):
        weight = jnp.where(routes[:, k : k + 1] == expert, given[:, k : k + 1], weight)
    slot = 3 * ((line >> 1) & 1) + (line >> 2)
    weight = jnp.where(named & (rank == slot), weight, 0.0)
    rows = weight.shape[0]
    at = 0
    for part in three_parts(weight):
        for side in range(2):
            out_ref[at : at + rows] = jnp.where((line & 1) == side, part, 0.0).astype(bf16)
            at += rows


def swap_kernel(
    core_ref,
    both_ref,
    gain_ref,
    gate_ref,
    up_ref,
    shared_gate_ref,
    shared_up_ref,
    routes_ref,
    weights_ref,
    out_gain_ref,
    outgoing_ref,
    swap_ref,
    keep_ref,
    combine_ref,
    later_gain_ref,
    own_gain,
    shared_gate,
    shared_up,
    routes,
    weights,
    sems,
):
    depth = gate_ref.shape[0]
    pairs = (
        (routes_ref, routes),
        (weights_ref, weights),
        (gain_ref, own_gain),
        (shared_gate_ref, shared_gate),
        (shared_up_ref, shared_up),
        (out_gain_ref, later_gain_ref),
        (gate_ref, swap_ref.at[:depth]),
        (up_ref, swap_ref.at[depth : 2 * depth]),
    )
    copies = [pltpu.make_async_copy(a, b, sems.at[n]) for n, (a, b) in enumerate(pairs)]
    for copy in copies:
        copy.start()
    core = core_ref[0]
    first = core == 0
    for copy in copies[:3]:
        copy.wait()
    outgoing_ref[...] = packed(core, routes[...].T, both_ref, outgoing_ref.shape[0])
    combine_weights(routes, weights, combine_ref)
    gain = own_gain[...]
    rows = (both_ref[core].astype(f32) * gain).astype(bf16)
    half = rows.shape[0] // 2
    parts = three_parts(gain)
    line = iota((8, gain.shape[1]), 0)
    gain = jnp.where(line == 0, parts[0], jnp.where(line == 1, parts[1], parts[2]))
    gain = jnp.where(line < 3, gain, 0.0).astype(bf16)
    swap_ref[2 * depth + 2 * half :] = jnp.concatenate([gain] * 4, axis=1)
    for copy in copies[3:5]:
        copy.wait()
    for n in range(keep_ref.shape[0]):
        cut = slice(n * 128, (n + 1) * 128)
        part = dot(rows, jnp.concatenate([shared_gate[:, cut], shared_up[:, cut]], axis=1))
        keep_ref[n] = jnp.where(first, part[:half], part[half:])
        at, lane = 2 * depth + n // 4 * half, n % 4 * 256
        swap_ref[at : at + half, lane : lane + 256] = jnp.where(
            first, part[half:], part[:half]
        ).astype(bf16)
    for copy in copies[5:]:
        copy.wait()


def hidden_parts_kernel(
    core_ref,
    rows_ref,
    both_ref,
    gain_ref,
    near_ref,
    far_ref,
    kept_ref,
    out_ref,
    wide,
):
    first = core_ref[0] == 0
    slots = rows_ref.shape[0] // 4
    wide[...] = rows_ref[...].astype(f32)
    own, other = (
        jnp.concatenate([wide[pl.ds(q, slots, stride=4), :] for q in pair], axis=1)
        for pair in ((0, 1), (2, 3))
    )
    squares = jnp.sum(own * own + other * other, axis=1, keepdims=True)
    low, high = both_ref[0].astype(f32), both_ref[1].astype(f32)
    token_squares = jnp.sum(low * low + high * high, axis=1, keepdims=True)
    half = token_squares.shape[0] // 2
    token_squares = jnp.where(first, token_squares[:half], token_squares[half:])
    squares = jnp.concatenate([squares, token_squares], axis=0) * (1.0 / D)
    parts = three_parts(to_row(squares, 256))
    line = iota((8, 256), 0)
    extra = jnp.where(line == 0, parts[0], jnp.where(line == 1, parts[1], parts[2]))
    extra = jnp.where(line < 3, extra, 0.0).astype(bf16)
    own = (own * gain_ref[...]).astype(bf16)
    depth = gain_ref.shape[1]
    shared_at = 2 * depth
    swapped = far_ref[shared_at + 2 * half :, :depth].astype(f32)
    gain_other = swapped[0:1] + swapped[1:2] + swapped[2:3]
    other = (other * gain_other).astype(bf16)
    for n in range(out_ref.shape[0]):
        cut = slice(n * 128, (n + 1) * 128)
        near = jnp.concatenate([near_ref[:depth, cut], near_ref[depth:shared_at, cut]], axis=1)
        far = jnp.concatenate([far_ref[:depth, cut], far_ref[depth:shared_at, cut]], axis=1)
        out_ref[n, :slots] = (dot(own, near) + dot(other, far)).astype(bf16)
        at, lane = shared_at + n // 4 * half, n % 4 * 256
        given = far_ref[at : at + half, lane : lane + 256].astype(f32)
        out_ref[n, slots : slots + half] = (kept_ref[n] + given).astype(bf16)
        out_ref[n, slots + half :] = extra


def hidden_kernel(parts_ref, out_ref):
    rows = out_ref.shape[0]
    total = parts_ref[0].astype(f32)
    for n in range(1, parts_ref.shape[0]):
        total = total + parts_ref[n].astype(f32)
    mean = total[rows : rows + 1] + total[rows + 1 : rows + 2] + total[rows + 2 : rows + 3]
    scale = to_column(lax.rsqrt(mean + EPS), rows)
    gate = jnp.where(scale > 0.0, total[:rows, :128] * scale, 0.0)
    up = jnp.where(scale > 0.0, total[:rows, 128:] * scale, 0.0)
    out_ref[...] = (gate / (1.0 + jnp.exp(-gate)) * up).astype(bf16)


def lanes_of(ref, core, lo, hi):
    return jnp.concatenate([ref[n, lo:hi] for n in range(core, ref.shape[0], 2)], axis=1)


def down_kernel(hidden_ref, down_ref, shared_down_ref, out_ref, shared_ref, wide):
    slots = out_ref.shape[0] // 4
    down = down_ref[...]
    for core in range(2):
        rows = dot(lanes_of(hidden_ref, core, 0, slots), down)
        for side in range(2):
            wide[pl.ds(2 * core + side, slots, stride=4), :] = rows[
                :, side * 128 : (side + 1) * 128
            ]
    out_ref[...] = wide[...].astype(bf16)
    end = hidden_ref.shape[1]
    hidden = jnp.concatenate(
        [lanes_of(hidden_ref, core, slots, end) for core in range(2)], axis=0
    )
    shared_ref[...] = dot(hidden, shared_down_ref[...])


def combine_kernel(rows_ref, weights_ref, shared_ref, mixed_ref, squares_ref):
    parts = dot(weights_ref[...], rows_ref[...])
    count = shared_ref.shape[0]
    low, high = (
        sum(parts[at * count : (at + 1) * count] for at in (side, side + 2, side + 4))
        for side in range(2)
    )
    mixed = shared_ref[...] + jnp.concatenate([low, high], axis=1)
    mixed_ref[...] = mixed
    squares = to_row(jnp.sum(mixed * mixed, axis=1, keepdims=True), 128)
    squares_ref[...] = jnp.broadcast_to(squares[None], squares_ref.shape)


def norm_kernel(squares_ref, mixed_ref, gain_ref, out_ref):
    total = jnp.sum(squares_ref[...], axis=0)
    scale = to_column(lax.rsqrt(total / D + EPS), out_ref.shape[0])
    out_ref[...] = (mixed_ref[...] * scale * gain_ref[...]).astype(bf16)


def call(body, out, *operands, flops=0, far=(), scratch=()):
    def spec(n, array):
        if n in far:
            return pl.BlockSpec(memory_space=pltpu.HBM)
        return pl.BlockSpec(memory_space=pltpu.SMEM if array.shape == (1,) else pltpu.VMEM)

    operands = [
        pltpu.with_memory_space_constraint(a, pltpu.HBM) if n in far else a
        for n, a in enumerate(operands)
    ]
    outs = out if isinstance(out, tuple) else (out,)
    specs = tuple(pl.BlockSpec(memory_space=pltpu.VMEM) for _ in outs)
    moved = sum(a.size * a.dtype.itemsize for a in (*operands, *outs))
    return pl.pallas_call(
        body,
        out_shape=out,
        in_specs=[spec(n, a) for n, a in enumerate(operands)],
        out_specs=specs if isinstance(out, tuple) else specs[0],
        scratch_shapes=scratch,
        compiler_params=pltpu.CompilerParams(vmem_limit_bytes=24 * MIB),
        cost_estimate=pl.CostEstimate(flops=flops, bytes_accessed=moved, transcendentals=0),
    )(*operands)


def shape(dims, dtype):
    return jax.ShapeDtypeStruct(dims, dtype)


def exchanged(rows, sources):
    blocks = rows.reshape(sources, -1, 4, 128)
    return lax.all_to_all(blocks, "ep", 0, 0, tiled=True).reshape(rows.shape)


def per_device(
    tokens,
    norm_gain,
    routes,
    route_weights,
    gate_proj,
    up_proj,
    down_proj,
    shared_gate,
    shared_up,
    shared_down,
    out_gain,
):
    rows, features = tokens.shape
    sources, lines, cores = (lax.axis_size(a) for a in ("ep", "x", "core"))
    sent = sources * 12
    slots = sources * 3
    half = rows // 2
    core = lax.axis_index("core").astype(i32).reshape(1)
    swap = [(0, 1), (1, 0)]
    gain = norm_gain.reshape(1, features)
    gate, up, down = gate_proj[0], up_proj[0], down_proj[0]

    routes, route_weights = routes.T, route_weights.T
    both = lax.all_gather(tokens, "core", axis=0)
    outgoing, near, kept, weights, later_gain = call(
        swap_kernel,
        (
            shape((sent, 128), bf16),
            shape((2 * features + 2 * half + 8, 1024), bf16),
            shape((lines, half, 256), f32),
            shape((6 * rows, sent), bf16),
            shape((1, features), f32),
        ),
        core,
        both,
        gain,
        gate,
        up,
        shared_gate,
        shared_up,
        routes,
        route_weights,
        out_gain.reshape(1, features),
        flops=2 * rows * features * 2048,
        far=range(2, 10),
        scratch=[
            pltpu.VMEM((1, features), f32),
            pltpu.VMEM((features, 1024), bf16),
            pltpu.VMEM((features, 1024), bf16),
            pltpu.VMEM(routes.shape, i32),
            pltpu.VMEM(route_weights.shape, f32),
            pltpu.SemaphoreType.DMA((8,)),
        ],
    )
    far = lax.ppermute(near, "core", swap)
    arrived = exchanged(outgoing, sources)

    parts = call(
        hidden_parts_kernel,
        shape((lines, slots + half + 8, 256), bf16),
        core,
        arrived,
        both,
        gain,
        near,
        far,
        kept,
        flops=4 * slots * features * 2048,
        scratch=[pltpu.VMEM((sent, 128), f32)],
    )
    parts = lax.all_to_all(parts, "x", 0, 0, tiled=True)
    hidden = call(hidden_kernel, shape((slots + half, 128), bf16), parts)
    hidden = lax.all_gather(hidden, ("x", "core"), axis=0)
    leaving, shared = call(
        down_kernel,
        (shape((sent, 128), bf16), shape((rows, features), f32)),
        hidden,
        down,
        shared_down,
        scratch=[pltpu.VMEM((sent, 128), f32)],
        flops=4 * slots * 1024 * features,
    )
    returned = exchanged(leaving, sources)
    mixed, squares = call(
        combine_kernel,
        (shape((rows, features), f32), shape((lines * cores, 1, 128), f32)),
        returned,
        weights,
        shared,
    )
    squares = lax.all_to_all(squares, ("x", "core"), 0, 0, tiled=True)
    return call(norm_kernel, shape((rows, features), bf16), squares, mixed, later_gain)


def solution(mesh):
    sources, members = mesh.devices.shape
    inner = Mesh(mesh.devices.reshape(sources, members // 2, 2), ("ep", "x", "core"))
    tp = ("x", "core")
    return jax.shard_map(
        per_device,
        mesh=inner,
        in_specs=(
            P("ep", tp),
            P(tp),
            P("ep", None),
            P("ep", None),
            P("ep", tp, None),
            P("ep", tp, None),
            P("ep", None, tp),
            P(tp, None),
            P(tp, None),
            P(None, tp),
            P(tp),
        ),
        out_specs=P("ep", tp),
        check_vma=False,
    )
```
